1024 devices in a mesh: rep: 2 (over z_hi), fs: 64 (over z_lo, y), tp: 8 (over x, core).
Axes of the slice: x: 4, y: 8, z: 16 (z_hi: 2, z_lo: 8; z = z_hi * 8 + z_lo), core: 2. Of those that a mesh axis runs over, the one named last changes fastest.
Arguments:
- tokens: bfloat16 [65536, 2048], P(('rep', 'fs')), may hold values from -6 to 6
- norm_gain: float32 [2048], replicated, may hold values from 0.1 to 1.9
- up_weight: bfloat16 [2048, 4096], P('fs', 'tp'), may hold values from -0.125 to 0.125
- down_weight: bfloat16 [4096, 2048], P('tp', 'fs'), may hold values from -0.09375 to 0.09375
Outputs:
- result: bfloat16 [65536, 2048], P(('rep', 'fs', 'tp'))
The draws below stay inside these ranges and needn't reach their ends.
All inputs are finite; a program needn't handle non-finite values.
Results may differ from the reference program's by a relative error of at most 0.012.
Values may be sent and summed in bfloat16 or wider, within the bound.
No kernel may reach another device: no remote copies, remote signals or barrier semaphores. Data moves between devices by JAX's collectives and lax.ppermute only.
A program may use at most 64 MiB of HBM per device.

```python
import jax
import jax.numpy as jnp
from jax import lax

D = 2048
FF = 4096
TOKENS = 65536
N_TP = 8


def block_scale(own_key, dims, split, smallest, largest):
    loudness = 1.0
    for axis_at, parts in split:
        draws = jax.random.uniform(jax.random.fold_in(jax.random.fold_in(own_key, 6), axis_at), (parts,), jnp.float32, smallest / len(split), largest / len(split))
        loudness = loudness * jnp.repeat(jnp.exp(draws), dims[axis_at] // parts).reshape((-1,) + (1,) * (len(dims) - 1 - axis_at))
    return loudness


def normal_values(key, shape, spread, most, pieces=(), held_as=jnp.bfloat16):
    level = block_scale(key, shape, pieces, -0.22, 0.18) if pieces else 1.0
    drawn = jax.random.normal(key, shape, jnp.float32) * spread * level
    return jnp.minimum(jnp.maximum(drawn, -most), most).astype(held_as)


def setup_inputs(seed: int = 0) -> dict:
    key_list = jax.random.split(jax.random.key(seed), 5)
    return {
        "tokens": normal_values(key_list[0], (TOKENS, D), 1.0, 6.0, ((0, 128),)),
        "norm_gain": jnp.clip(1.0 + 0.18 * jax.random.normal(key_list[1], (D,), jnp.float32), 0.1, 1.9),
        "up_weight": normal_values(key_list[2], (D, FF), D ** -0.5, 0.125, ((0, 64), (1, 8))),
        "down_weight": normal_values(key_list[3], (FF, D), FF ** -0.5, 0.09375, ((0, 8), (1, 64))),
    }


EPS = 1e-06

def reference(tokens, norm_gain, up_weight, down_weight):
    xf = tokens.astype(jnp.float32)
    scale = lax.rsqrt(lax.optimization_barrier(jnp.mean(xf * xf, axis=-1, keepdims=True)) + EPS)
    normed = (xf * scale * norm_gain.astype(jnp.float32)).astype(jnp.bfloat16)
    lifted = jnp.dot(normed, up_weight, preferred_element_type=jnp.float32)
    hidden = jnp.square(jnp.maximum(lifted, 0.0)).astype(jnp.bfloat16)
    block = FF // N_TP
    total = xf
    for index in range(N_TP):
        part = jnp.dot(hidden[:, index * block:(index + 1) * block], down_weight[index * block:(index + 1) * block, :], preferred_element_type=jnp.float32)
        rounded = lax.optimization_barrier(part.astype(jnp.bfloat16))
        total = total + rounded.astype(jnp.float32)
    return total.astype(jnp.bfloat16)
```

```python
import jax
import jax.numpy as jnp
from jax import lax
from jax.experimental import pallas as pl
from jax.experimental.pallas import tpu as pltpu
from jax.sharding import Mesh
from jax.sharding import PartitionSpec as P

EPS = 1e-06
REP, Z, Y, X, CORE = 2, 8, 8, 4, 2
UP_STEPS = (("y", 4), ("z", 4), ("y", 2), ("z", 2), ("y", 1), ("z", 1))
DOWN_STEPS = (("z", 4), ("y", 4), ("z", 2), ("y", 2), ("z", 1), ("y", 1))


def from_side(array, axis, shift):
    names, size = (("y", "core"), Y) if axis == "y" else (("rep", "z", "core"), REP * Z)
    pairs = []
    for i in range(size):
        pairs.append(((i + shift) % size * 2, i * 2))
        pairs.append(((i - shift) % size * 2 + 1, i * 2 + 1))
    return lax.ppermute(array, names, pairs)


def offsets(steps):
    laid = [(0, 0)]
    for axis, shift in steps:
        dz, dy = (shift, 0) if axis == "z" else (0, shift)
        laid = laid + [(z + dz, y + dy) for z, y in laid]
    return laid


def doubled(up, down):
    for k in range(len(UP_STEPS)):
        up_in = from_side(up, *UP_STEPS[k])
        down_in = from_side(down, *DOWN_STEPS[k])
        if k + 1 == len(UP_STEPS):
            return (up, up_in), (down, down_in)
        up = jnp.concatenate([up, up_in])
        down = jnp.concatenate([down, down_in])


def place(place_ref, halves, laid, whole):
    z, y, sign = place_ref[0], place_ref[1], place_ref[3]
    half = len(laid) // 2
    for j, (dz, dy) in enumerate(laid):
        at = ((z + sign * dz) & (Z - 1)) * Y + ((y + sign * dy) & (Y - 1))
        rows = pl.ds(pl.multiple_of(at * 32, 32), 32)
        whole[rows, :] = halves[j // half][j % half]


def product_kernel(
    place_ref, normed, up_a, up_b, down_a, down_b, theirs, own, up, down, hidden
):
    place(place_ref, (up_a, up_b), offsets(UP_STEPS), up)
    place(place_ref, (down_a, down_b), offsets(DOWN_STEPS), down)
    core = place_ref[2]

    @pl.loop(0, 2)
    def _(n):
        columns = pl.ds(pl.multiple_of(n * 256, 256), 256)
        lifted = jnp.dot(
            normed[...], up[:, columns], preferred_element_type=jnp.float32
        )
        active = jnp.square(jnp.maximum(lifted, 0.0)).astype(jnp.bfloat16)
        for j in range(X * CORE):
            x, c = divmod(j, CORE)
            side = jnp.where(core == c, 256, 0)
            rows = pl.ds(pl.multiple_of(side + x * 64, 64), 64)
            hidden[rows, columns] = active[j * 64 : (j + 1) * 64]

    @pl.loop(0, 8)
    def _(n):
        columns = pl.ds(pl.multiple_of(n * 256, 256), 256)
        part = lax.dot_general(
            hidden[...],
            down[columns, :],
            (((1,), (1,)), ((), ())),
            preferred_element_type=jnp.float32,
        ).astype(jnp.bfloat16)
        theirs[:, columns] = part[:256]
        own[:, columns] = part[256:]


def products(where, normed, up, down):
    block = pl.BlockSpec(memory_space=pltpu.VMEM)
    out = jax.ShapeDtypeStruct((256, 2048), jnp.bfloat16)
    return pl.pallas_call(
        product_kernel,
        out_shape=(out, out),
        in_specs=[pl.BlockSpec(memory_space=pltpu.SMEM)] + [block] * 5,
        out_specs=(block, block),
        scratch_shapes=[
            pltpu.VMEM((2048, 512), jnp.bfloat16),
            pltpu.VMEM((2048, 512), jnp.bfloat16),
            pltpu.VMEM((512, 512), jnp.bfloat16),
        ],
        compiler_params=pltpu.CompilerParams(vmem_limit_bytes=40 * 2**20),
        cost_estimate=pl.CostEstimate(
            flops=2**32, bytes_accessed=8 * 2**20, transcendentals=0
        ),
    )(where, normed, *up, *down)


def shards(tokens, norm_gain, up_weight, down_weight):
    core = lax.axis_index("core")
    up, down = doubled(up_weight[None], down_weight.T[None])
    xf = tokens.astype(jnp.float32)
    scale = lax.rsqrt(jnp.mean(xf * xf, axis=-1, keepdims=True) + EPS)
    normed = (xf * scale * norm_gain).astype(jnp.bfloat16)
    where = jnp.stack(
        [lax.axis_index("z"), lax.axis_index("y"), core, 1 - 2 * core]
    ).astype(jnp.int32)
    theirs, own = products(where, normed, up, down)
    beside = lax.ppermute(theirs, "core", [(0, 1), (1, 0)])
    pair = (own.astype(jnp.float32) + beside.astype(jnp.float32)).astype(jnp.bfloat16)
    parts = lax.all_to_all(pair.reshape(X, 64, 2048), "x", 0, 0, tiled=True)
    mine = lax.axis_index("x") * CORE + core
    residual = lax.dynamic_slice_in_dim(tokens, mine * 64, 64, 0)
    summed = jnp.sum(parts.astype(jnp.float32), axis=0)
    return (residual.astype(jnp.float32) + summed).astype(jnp.bfloat16)


def solution(mesh):
    torus = Mesh(
        mesh.devices.reshape(REP, Z, Y, X, CORE), ("rep", "z", "y", "x", "core")
    )
    rep_fs = ("rep", "z", "y")
    tp = ("x", "core")
    in_specs = (P(rep_fs, None), P(), P(("z", "y"), tp), P(tp, ("z", "y")))
    return jax.shard_map(
        shards,
        mesh=torus,
        in_specs=in_specs,
        out_specs=P(rep_fs + tp, None),
        check_vma=False,
    )
```

```python
import jax
import jax.numpy as jnp
from jax import lax
from jax.experimental import pallas as pl
from jax.experimental.pallas import tpu as pltpu
from jax.sharding import Mesh
from jax.sharding import PartitionSpec as P


EPS = 1e-06
REP, Z, Y, X, CORE = 2, 8, 8, 4, 2
VMEM = pl.BlockSpec(memory_space=pltpu.VMEM)
SMEM = pl.BlockSpec(memory_space=pltpu.SMEM)


def steps_of(shift):
    return ((0, shift), (shift, 0), (shift, shift))


def from_side(array, dz, dy):
    deep = REP * Z
    pairs = []
    for z in range(deep):
        for y in range(Y):
            for core, sign in ((0, 1), (1, -1)):
                source = ((z + sign * dz) % deep * Y + (y + sign * dy) % Y) * 2 + core
                pairs.append((source, (z * Y + y) * 2 + core))
    return lax.ppermute(array, ("rep", "z", "y", "core"), pairs)


def offsets(shifts):
    laid = [(0, 0)]
    for shift in shifts:
        laid = [
            (z + dz, y + dy) for dz, dy in ((0, 0), *steps_of(shift)) for z, y in laid
        ]
    return laid


HELD = offsets((4, 2))
CLASSES = ((0, 0), *steps_of(1))


def join_kernel(*refs):
    ins, outs = refs[:4], refs[4:]
    for k, piece in enumerate(ins):
        n = piece.shape[1]
        for both in range(2):
            if len(outs) == 1:
                outs[0][both, k * n : (k + 1) * n] = piece[both]
            else:
                outs[both][k * n : (k + 1) * n] = piece[both]


def join(pieces, apart):
    n = pieces[0].shape[1] * 4
    if apart:
        out = (jax.ShapeDtypeStruct((n, 32, 512), jnp.bfloat16),) * 2
        specs = (VMEM, VMEM)
    else:
        out = jax.ShapeDtypeStruct((2, n, 32, 512), jnp.bfloat16)
        specs = VMEM
    return pl.pallas_call(
        join_kernel,
        out_shape=out,
        in_specs=[VMEM] * 4,
        out_specs=specs,
        compiler_params=pltpu.CompilerParams(vmem_limit_bytes=8 * 2**20),
    )(*pieces)


def pair_kernel(up, down, out):
    out[0, 0] = up[...]
    out[1, 0] = down[...]


def pair(up, down):
    return pl.pallas_call(
        pair_kernel,
        out_shape=jax.ShapeDtypeStruct((2, 1, 32, 512), jnp.bfloat16),
        in_specs=[VMEM, VMEM],
        out_specs=VMEM,
        compiler_params=pltpu.CompilerParams(vmem_limit_bytes=2**20),
    )(up, down)


def place(where, pieces, classes, whole, halved):
    z, y, sign = where[0], where[1], where[3]
    for piece, (cz, cy) in zip(pieces, classes, strict=True):
        for j, (dz, dy) in enumerate(HELD):
            at_z = (z + sign * (dz + cz)) & (Z - 1)
            at_y = (y + sign * (dy + cy)) & (Y - 1)
            at = ((at_z >> 1) if halved else at_z) * Y + at_y
            whole[pl.ds(pl.multiple_of(at * 32, 32), 32), :] = piece[j]


def down_product(hidden, down, theirs, own):
    @pl.loop(0, 4)
    def _(n):
        columns = pl.ds(pl.multiple_of(n * 256, 256), 256)
        part = lax.dot_general(
            hidden[...],
            down[columns, :],
            (((1,), (1,)), ((), ())),
            preferred_element_type=jnp.float32,
        ).astype(jnp.bfloat16)
        theirs[:, columns] = part[:256]
        own[:, columns] = part[256:]


def first_kernel(
    where, normed, u0, u1, u2, u3, d0, d1, theirs, own, hidden, up, down
):
    place(where, (u0, u1, u2, u3), CLASSES, up, False)
    core = where[2]

    @pl.loop(0, 2)
    def _(n):
        columns = pl.ds(pl.multiple_of(n * 256, 256), 256)
        lifted = jnp.dot(
            normed[...], up[:, columns], preferred_element_type=jnp.float32
        )
        active = jnp.square(jnp.maximum(lifted, 0.0)).astype(jnp.bfloat16)
        for j in range(X * CORE):
            x, c = divmod(j, CORE)
            side = jnp.where(core == c, 256, 0)
            rows = pl.ds(pl.multiple_of(side + x * 64, 64), 64)
            hidden[rows, columns] = active[j * 64 : (j + 1) * 64]

    place(where, (d0, d1), CLASSES[:2], down, True)
    down_product(hidden, down, theirs, own)


def second_kernel(where, hidden, d2, d3, theirs, own, down):
    place(where, (d2, d3), CLASSES[2:], down, True)
    down_product(hidden, down, theirs, own)


def products(where, normed, up, down):
    out = jax.ShapeDtypeStruct((256, 1024), jnp.bfloat16)
    early_call = pl.pallas_call(
        first_kernel,
        out_shape=(out, out, jax.ShapeDtypeStruct((512, 512), jnp.bfloat16)),
        in_specs=[SMEM] + [VMEM] * 7,
        out_specs=(VMEM,) * 3,
        scratch_shapes=[
            pltpu.VMEM((2048, 512), jnp.bfloat16),
            pltpu.VMEM((1024, 512), jnp.bfloat16),
        ],
        compiler_params=pltpu.CompilerParams(vmem_limit_bytes=32 * 2**20),
        cost_estimate=pl.CostEstimate(
            flops=3 * 2**29, bytes_accessed=6 * 2**20, transcendentals=0
        ),
    )
    late_call = pl.pallas_call(
        second_kernel,
        out_shape=(out, out),
        in_specs=[SMEM] + [VMEM] * 3,
        out_specs=(VMEM,) * 2,
        scratch_shapes=[pltpu.VMEM((1024, 512), jnp.bfloat16)],
        compiler_params=pltpu.CompilerParams(vmem_limit_bytes=16 * 2**20),
        cost_estimate=pl.CostEstimate(
            flops=2**29, bytes_accessed=2 * 2**20, transcendentals=0
        ),
    )
    theirs, own, hidden = early_call(where, normed, *up, *down[:2])
    late = late_call(where, hidden, *down[2:])
    return (theirs, own), late


def over_tp(theirs, own):
    beside = lax.ppermute(theirs, "core", [(0, 1), (1, 0)])
    both = (own.astype(jnp.float32) + beside.astype(jnp.float32)).astype(jnp.bfloat16)
    return lax.all_to_all(both.reshape(X, 64, 1024), "x", 0, 0, tiled=True)


def last_kernel(where, residual, first, second, out):
    odd = where[0] & 1
    for side, parts in ((0, first), (1, second)):
        parity = odd ^ side
        for k in range(4):
            columns = pl.ds(pl.multiple_of((2 * k + parity) * 256, 256), 256)
            here = slice(k * 256, (k + 1) * 256)
            total = residual[:, columns].astype(jnp.float32)
            for x in range(X):
                total = total + parts[x, :, here].astype(jnp.float32)
            out[:, columns] = total.astype(jnp.bfloat16)


def last(where, residual, first, second):
    return pl.pallas_call(
        last_kernel,
        out_shape=jax.ShapeDtypeStruct((64, 2048), jnp.bfloat16),
        in_specs=[SMEM] + [VMEM] * 3,
        out_specs=VMEM,
        compiler_params=pltpu.CompilerParams(vmem_limit_bytes=8 * 2**20),
    )(where, residual, first, second)


def shards(tokens, norm_gain, up_weight, down_weight):
    core = lax.axis_index("core")
    held = pair(up_weight, down_weight.T)
    held = join([held] + [from_side(held, *step) for step in steps_of(4)], False)
    up, down = join([held] + [from_side(held, *step) for step in steps_of(2)], True)
    ups = [up] + [from_side(up, *step) for step in steps_of(1)]
    downs = [down]
    for step in steps_of(1):
        downs.append(from_side(down, *step))
    xf = tokens.astype(jnp.float32)
    scale = lax.rsqrt(jnp.mean(xf * xf, axis=-1, keepdims=True) + EPS)
    normed = (xf * scale * norm_gain).astype(jnp.bfloat16)
    where = jnp.stack(
        [lax.axis_index("z"), lax.axis_index("y"), core, 1 - 2 * core]
    ).astype(jnp.int32)
    first, second = products(where, normed, ups, downs)
    mine = lax.axis_index("x") * CORE + core
    residual = lax.dynamic_slice_in_dim(tokens, mine * 64, 64, 0)
    return last(where, residual, over_tp(*first), over_tp(*second))


def solution(mesh):
    torus = Mesh(
        mesh.devices.reshape(REP, Z, Y, X, CORE), ("rep", "z", "y", "x", "core")
    )
    rep_fs = ("rep", "z", "y")
    tp = ("x", "core")
    in_specs = (P(rep_fs, None), P(), P(("z", "y"), tp), P(tp, ("z", "y")))
    return jax.shard_map(
        shards,
        mesh=torus,
        in_specs=in_specs,
        out_specs=P(rep_fs + tp, None),
        check_vma=False,
    )
```

```python
import jax
import jax.numpy as jnp
from jax import lax
from jax.experimental import pallas as pl
from jax.experimental.pallas import tpu as pltpu
from jax.sharding import Mesh
from jax.sharding import PartitionSpec as P


EPS = 1e-06
REP, Z, Y, X, CORE = 2, 8, 8, 4, 2
VMEM = pl.BlockSpec(memory_space=pltpu.VMEM)
SMEM = pl.BlockSpec(memory_space=pltpu.SMEM)


UP_STEPS = (("y", 4), ("z", 4), ("y", 2), ("z", 2), ("z", 1), ("y", 1))
DOWN_STEPS = (("y", 4), ("z", 4), ("z", 2), ("y", 2), ("y", 1), ("z", 1))


def from_side(array, axis, shift):
    names, size = (("y", "core"), Y) if axis == "y" else (("rep", "z", "core"), REP * Z)
    pairs = []
    for i in range(size):
        pairs.append(((i + shift) % size * 2, i * 2))
        pairs.append(((i - shift) % size * 2 + 1, i * 2 + 1))
    return lax.ppermute(array, names, pairs)


def along_x(array, forward):
    pairs = []
    for x in range(X):
        pairs.append((x * 2, (x + forward) % X * 2))
        pairs.append((x * 2 + 1, (x - forward) % X * 2 + 1))
    return lax.ppermute(array, ("x", "core"), pairs)


def offsets(steps):
    laid = [(0, 0)]
    for axis, shift in steps:
        dz, dy = (shift, 0) if axis == "z" else (0, shift)
        laid = laid + [(z + dz, y + dy) for z, y in laid]
    return laid


def kernel_call(kernel, outs, n_vmem, scratch=(), smem=True, mib=8, flops=0, **rest):
    single = not isinstance(outs, tuple)
    return pl.pallas_call(
        kernel,
        out_shape=outs,
        in_specs=([SMEM] if smem else []) + [VMEM] * n_vmem,
        out_specs=VMEM if single else (VMEM,) * len(outs),
        scratch_shapes=[pltpu.VMEM(s, jnp.bfloat16) for s in scratch],
        compiler_params=pltpu.CompilerParams(vmem_limit_bytes=mib * 2**20),
        cost_estimate=pl.CostEstimate(
            flops=flops, bytes_accessed=2**20, transcendentals=0
        )
        if flops
        else None,
        **rest,
    )


def bf16(*shape):
    return jax.ShapeDtypeStruct(shape, jnp.bfloat16)


def pair_kernel(up, down, out, sem):
    first = pltpu.make_async_copy(up, out.at[0, 0], sem.at[0])
    second = pltpu.make_async_copy(down, out.at[1, 0], sem.at[1])
    first.start()
    second.start()
    first.wait()
    second.wait()


def pair(up, down):
    return pl.pallas_call(
        pair_kernel,
        out_shape=bf16(2, 1, 32, 512),
        in_specs=[pl.BlockSpec(memory_space=pltpu.HBM)] * 2,
        out_specs=VMEM,
        scratch_shapes=[pltpu.SemaphoreType.DMA((2,))],
        compiler_params=pltpu.CompilerParams(vmem_limit_bytes=2**20),
    )(up, down)


def join_kernel(a, b, out):
    n = a.shape[0]
    out[:n] = a[...]
    out[n:] = b[...]


def join(a, b):
    n = a.shape[0]
    return kernel_call(join_kernel, bf16(2 * n, 32, 512), 2, smem=False)(a, b)


def join_both_kernel(a, b, out):
    n = a.shape[1]
    out[:, :n] = a[...]
    out[:, n:] = b[...]


def join_both(a, b):
    n = a.shape[1]
    return kernel_call(join_both_kernel, bf16(2, 2 * n, 32, 512), 2, smem=False)(a, b)


def join_apart_kernel(a, b, up, down):
    n = a.shape[1]
    for k, out in enumerate((up, down)):
        out[:n] = a[k]
        out[n:] = b[k]


def join_apart(a, b):
    out = bf16(2 * a.shape[1], 32, 512)
    return kernel_call(join_apart_kernel, (out, out), 2, smem=False)(a, b)


def place(where, piece, laid, whole, halved):
    z, y, sign = where[0], where[1], where[3]
    for j, (dz, dy) in enumerate(laid):
        at_z = (z + sign * dz) & (Z - 1)
        at_y = (y + sign * dy) & (Y - 1)
        at = ((at_z >> 1) if halved else at_z) * Y + at_y
        whole[pl.ds(pl.multiple_of(at * 32, 32), 32), :] = piece[j]


def down_product(hidden, down, theirs, own, part):
    @pl.loop(0, 4)
    def _(n):
        columns = pl.ds(pl.multiple_of(n * 256, 256), 256)
        made = lax.dot_general(
            hidden[...],
            down[columns, :],
            (((1,), (1,)), ((), ())),
            preferred_element_type=jnp.float32,
        ).astype(jnp.bfloat16)
        theirs[part, :, columns] = made[:256]
        own[part, :, columns] = made[256:]


def early_kernel(where, normed, u0, u1, d0, theirs, own, hidden, up, down):
    laid = offsets(UP_STEPS)
    place(where, u0, laid[:32], up, False)
    place(where, u1, laid[32:], up, False)
    core = where[2]

    @pl.loop(0, 2)
    def _(n):
        columns = pl.ds(pl.multiple_of(n * 256, 256), 256)
        lifted = jnp.dot(
            normed[...], up[:, columns], preferred_element_type=jnp.float32
        )
        active = jnp.square(jnp.maximum(lifted, 0.0)).astype(jnp.bfloat16)
        for j in range(X * CORE):
            x, c = divmod(j, CORE)
            side = jnp.where(core == c, 256, 0)
            rows = pl.ds(pl.multiple_of(side + x * 64, 64), 64)
            hidden[rows, columns] = active[j * 64 : (j + 1) * 64]

    place(where, d0, offsets(DOWN_STEPS)[:32], down, True)
    down_product(hidden, down, theirs, own, 0)


def late_kernel(where, hidden, d1, theirs_in, own_in, theirs, own, down):
    place(where, d1, offsets(DOWN_STEPS)[32:], down, True)
    down_product(hidden, down, theirs, own, 1)


def add_kernel(where, own, beside, keep, ahead, back, far):
    x, sign = where[4], where[3]
    for out, step in ((far, 2), (back, -sign), (ahead, sign), (keep, 0)):
        rows = pl.ds(pl.multiple_of(((x + step) & (X - 1)) * 64, 64), 64)
        for part in range(2):
            total = own[part, rows].astype(jnp.float32)
            total = total + beside[part, rows].astype(jnp.float32)
            out[part] = total.astype(jnp.bfloat16)


def sum_kernel(a, b, out):
    out[...] = (a[...].astype(jnp.float32) + b[...].astype(jnp.float32)).astype(
        jnp.bfloat16
    )


def last_kernel(where, residual, a, b, c, out):
    odd = where[0] & 1
    for part in range(2):
        for k in range(4):
            at = (2 * k + (odd ^ part)) * 256
            columns = pl.ds(pl.multiple_of(at, 256), 256)
            here = slice(k * 256, (k + 1) * 256)
            total = residual[:, columns].astype(jnp.float32)
            for term in (a, b, c):
                total = total + term[part, :, here].astype(jnp.float32)
            out[:, columns] = total.astype(jnp.bfloat16)


def gathered(up_weight, down_weight):
    held = pair(up_weight, down_weight.T)
    held = join_both(held, from_side(held, *UP_STEPS[0]))
    up, down = join_apart(held, from_side(held, *UP_STEPS[1]))
    for k in range(2, 5):
        up_in = from_side(up, *UP_STEPS[k])
        down_in = from_side(down, *DOWN_STEPS[k])
        up, down = join(up, up_in), join(down, down_in)
    up_in = from_side(up, *UP_STEPS[5])
    down_in = from_side(down, *DOWN_STEPS[5])
    return (up, up_in), (down, down_in)


def over_tp(where, theirs, own, residual):
    beside = lax.ppermute(theirs, "core", [(0, 1), (1, 0)])
    piece = bf16(2, 64, 1024)
    keep, ahead, back, far = kernel_call(add_kernel, (piece,) * 4, 2)(
        where, own, beside
    )
    far_in = along_x(far, 1)
    back_in = along_x(back, -1)
    ahead = kernel_call(sum_kernel, piece, 2, smem=False)(ahead, far_in)
    ahead_in = along_x(ahead, 1)
    return kernel_call(last_kernel, bf16(64, 2048), 4)(
        where, residual, keep, back_in, ahead_in
    )


def shards(tokens, norm_gain, up_weight, down_weight):
    core, x = lax.axis_index("core"), lax.axis_index("x")
    (u0, u1), (d0, d1) = gathered(up_weight, down_weight)
    xf = tokens.astype(jnp.float32)
    scale = lax.rsqrt(jnp.mean(xf * xf, axis=-1, keepdims=True) + EPS)
    normed = (xf * scale * norm_gain).astype(jnp.bfloat16)
    where = jnp.stack(
        [lax.axis_index("z"), lax.axis_index("y"), core, 1 - 2 * core, x]
    ).astype(jnp.int32)
    residual = lax.dynamic_slice_in_dim(tokens, (x * CORE + core) * 64, 64, 0)
    out = bf16(2, 256, 1024)
    theirs, own, hidden = kernel_call(
        early_kernel,
        (out, out, bf16(512, 512)),
        4,
        scratch=((2048, 512), (1024, 512)),
        mib=14,
        flops=3 * 2**29,
    )(where, normed, u0, u1, d0)
    theirs, own = kernel_call(
        late_kernel,
        (out, out),
        4,
        scratch=((1024, 512),),
        mib=8,
        flops=2**29,
        input_output_aliases={3: 0, 4: 1},
    )(where, hidden, d1, theirs, own)
    return over_tp(where, theirs, own, residual)


def solution(mesh):
    torus = Mesh(
        mesh.devices.reshape(REP, Z, Y, X, CORE), ("rep", "z", "y", "x", "core")
    )
    rep_fs = ("rep", "z", "y")
    tp = ("x", "core")
    in_specs = (P(rep_fs, None), P(), P(("z", "y"), tp), P(tp, ("z", "y")))
    return jax.shard_map(
        shards,
        mesh=torus,
        in_specs=in_specs,
        out_specs=P(rep_fs + tp, None),
        check_vma=False,
    )
```

```python
import jax
import jax.numpy as jnp
from jax import lax
from jax.experimental import pallas as pl
from jax.experimental.pallas import tpu as pltpu
from jax.sharding import Mesh
from jax.sharding import PartitionSpec as P


EPS = 1e-06
REP, Z, Y, X, CORE = 2, 8, 8, 4, 2
VMEM = pl.BlockSpec(memory_space=pltpu.VMEM)
SMEM = pl.BlockSpec(memory_space=pltpu.SMEM)


UP_STEPS = ((0, 4), (4, 0), (0, 2), (2, 0))
DOWN_STEPS = ((0, 4), (4, 0), (2, 0), (0, 2))
CLASSES = ((0, 1), (1, 0), (1, 1))


def from_side(array, dz, dy):
    deep = REP * Z
    pairs = []
    for z in range(deep):
        for y in range(Y):
            for core, sign in ((0, 1), (1, -1)):
                source = ((z + sign * dz) % deep * Y + (y + sign * dy) % Y) * 2 + core
                pairs.append((source, (z * Y + y) * 2 + core))
    return lax.ppermute(array, ("rep", "z", "y", "core"), pairs)


def along_x(array, ahead):
    pairs = [(x, (x + ahead) % X) for x in range(X)]
    return lax.ppermute(array, "x", pairs)


def offsets(steps):
    laid = [(0, 0)]
    for dz, dy in steps:
        laid = laid + [(z + dz, y + dy) for z, y in laid]
    return laid


def shifted(steps, dz, dy):
    return [(z + dz, y + dy) for z, y in offsets(steps)]


def kernel_call(kernel, outs, n_vmem, scratch=(), smem=True, mib=8, flops=0, **rest):
    single = not isinstance(outs, tuple)
    return pl.pallas_call(
        kernel,
        out_shape=outs,
        in_specs=([SMEM] if smem else []) + [VMEM] * n_vmem,
        out_specs=VMEM if single else (VMEM,) * len(outs),
        scratch_shapes=[pltpu.VMEM(s, jnp.bfloat16) for s in scratch],
        compiler_params=pltpu.CompilerParams(vmem_limit_bytes=mib * 2**20),
        cost_estimate=pl.CostEstimate(
            flops=flops, bytes_accessed=2**20, transcendentals=0
        )
        if flops
        else None,
        **rest,
    )


def bf16(*shape):
    return jax.ShapeDtypeStruct(shape, jnp.bfloat16)


def pair_kernel(up, down, out, sem):
    first = pltpu.make_async_copy(up, out.at[0, 0], sem.at[0])
    second = pltpu.make_async_copy(down, out.at[1, 0], sem.at[1])
    first.start()
    second.start()
    first.wait()
    second.wait()


def pair(up, down):
    return pl.pallas_call(
        pair_kernel,
        out_shape=bf16(2, 1, 32, 512),
        in_specs=[pl.BlockSpec(memory_space=pl.ANY)] * 2,
        out_specs=VMEM,
        scratch_shapes=[pltpu.SemaphoreType.DMA((2,))],
        compiler_params=pltpu.CompilerParams(vmem_limit_bytes=63 * 2**20),
    )(up, down)


def join_kernel(a, b, out):
    n = a.shape[0]
    out[:n] = a[...]
    out[n:] = b[...]


def join(a, b):
    n = a.shape[0]
    return kernel_call(join_kernel, bf16(2 * n, 32, 512), 2, smem=False)(a, b)


def join_first_kernel(up, down, b, out):
    for k, own in enumerate((up, down)):
        out[k, 0] = own[...]
        out[k, 1] = b[k, 0]


def join_first(up, down, b):
    return kernel_call(join_first_kernel, bf16(2, 2, 32, 512), 3, smem=False)(
        up, down, b
    )


def join_apart_kernel(a, b, up, down):
    n = a.shape[1]
    for k, out in enumerate((up, down)):
        out[:n] = a[k]
        out[n:] = b[k]


def join_apart(a, b):
    out = bf16(2 * a.shape[1], 32, 512)
    return kernel_call(join_apart_kernel, (out, out), 2, smem=False)(a, b)


def place(where, piece, laid, whole, halved):
    z, y, sign = where[0], where[1], 1 - 2 * where[2]
    for j, (dz, dy) in enumerate(laid):
        at_z = (z + sign * dz) & (Z - 1)
        at_y = (y + sign * dy) & (Y - 1)
        at = ((at_z >> 1) if halved else at_z) * Y + at_y
        whole[pl.ds(pl.multiple_of(at * 32, 32), 32), :] = piece[j]


def down_product(hidden, down, theirs, own, part):
    @pl.loop(0, 4)
    def _(n):
        columns = pl.ds(pl.multiple_of(n * 256, 256), 256)
        made = lax.dot_general(
            hidden[...],
            down[columns, :],
            (((1,), (1,)), ((), ())),
            preferred_element_type=jnp.float32,
        ).astype(jnp.bfloat16)
        theirs[part, :, columns] = made[:256]
        own[part, :, columns] = made[256:]


def up_kernel(where, normed, u0, u1, u2, u3, hidden, up):
    for piece, shift in zip((u0, u1, u2, u3), ((0, 0), *CLASSES), strict=True):
        place(where, piece, shifted(UP_STEPS, *shift), up, False)
    core = where[2]

    @pl.loop(0, 2)
    def _(n):
        columns = pl.ds(pl.multiple_of(n * 256, 256), 256)
        lifted = jnp.dot(
            normed[...], up[:, columns], preferred_element_type=jnp.float32
        )
        active = jnp.square(jnp.maximum(lifted, 0.0)).astype(jnp.bfloat16)
        for j in range(X * CORE):
            x, c = divmod(j, CORE)
            side = jnp.where(core == c, 256, 0)
            rows = pl.ds(pl.multiple_of(side + x * 64, 64), 64)
            hidden[rows, columns] = active[j * 64 : (j + 1) * 64]


def early_kernel(where, hidden, d0, d1, theirs, own, down):
    place(where, d0, offsets(DOWN_STEPS), down, True)
    place(where, d1, shifted(DOWN_STEPS, *CLASSES[0]), down, True)
    down_product(hidden, down, theirs, own, 0)


def late_kernel(where, hidden, d2, d3, theirs_in, own_in, theirs, own, down):
    place(where, d2, shifted(DOWN_STEPS, *CLASSES[1]), down, True)
    place(where, d3, shifted(DOWN_STEPS, *CLASSES[2]), down, True)
    down_product(hidden, down, theirs, own, 1)


def add_kernel(where, own, beside, keep, ahead, back, far):
    x = where[3]
    for out, step in ((far, 2), (ahead, 1), (back, 3), (keep, 0)):
        rows = pl.ds(pl.multiple_of(((x + step) & (X - 1)) * 64, 64), 64)
        for part in range(2):
            total = own[part, rows].astype(jnp.float32)
            total = total + beside[part, rows].astype(jnp.float32)
            out[part] = total.astype(jnp.bfloat16)


def last_kernel(where, residual, a, b, c, d, out):
    odd = where[0] & 1
    for part in range(2):
        for k in range(4):
            at = (2 * k + (odd ^ part)) * 256
            columns = pl.ds(pl.multiple_of(at, 256), 256)
            here = slice(k * 256, (k + 1) * 256)
            total = residual[:, columns].astype(jnp.float32)
            for term in (a, b, c, d):
                total = total + term[part, :, here].astype(jnp.float32)
            out[:, columns] = total.astype(jnp.bfloat16)


def gathered(up_weight, down_weight):
    held_in = from_side(pair(up_weight, down_weight.T), *UP_STEPS[0])
    held = join_first(up_weight, down_weight.T, held_in)
    up, down = join_apart(held, from_side(held, *UP_STEPS[1]))
    for k in range(2, 4):
        up_in = from_side(up, *UP_STEPS[k])
        down_in = from_side(down, *DOWN_STEPS[k])
        up, down = join(up, up_in), join(down, down_in)
    ups, downs = [up], [down]
    for shift in CLASSES:
        ups.append(from_side(up, *shift))
    for shift in CLASSES:
        downs.append(from_side(down, *shift))
    return ups, downs


def over_tp(where, theirs, own, residual):
    beside = lax.ppermute(theirs, "core", [(0, 1), (1, 0)])
    piece = bf16(2, 64, 1024)
    keep, ahead, back, far = kernel_call(add_kernel, (piece,) * 4, 2)(
        where, own, beside
    )
    far, ahead, back = along_x(far, 2), along_x(ahead, 1), along_x(back, 3)
    return kernel_call(last_kernel, bf16(64, 2048), 5)(
        where, residual, keep, ahead, back, far
    )


def shards(tokens, norm_gain, up_weight, down_weight):
    core, x = lax.axis_index("core"), lax.axis_index("x")
    ups, downs = gathered(up_weight, down_weight)
    xf = tokens.astype(jnp.float32)
    scale = lax.rsqrt(jnp.mean(xf * xf, axis=-1, keepdims=True) + EPS)
    normed = (xf * scale * norm_gain).astype(jnp.bfloat16)
    where = jnp.stack([lax.axis_index("z"), lax.axis_index("y"), core, x]).astype(
        jnp.int32
    )
    residual = lax.dynamic_slice_in_dim(tokens, (x * CORE + core) * 64, 64, 0)
    hidden = kernel_call(
        up_kernel, bf16(512, 512), 5, scratch=((2048, 512),), mib=12, flops=2**30
    )(where, normed, *ups)
    out = bf16(2, 256, 1024)
    half = ((1024, 512),)
    theirs, own = kernel_call(
        early_kernel, (out, out), 3, scratch=half, flops=2**29
    )(where, hidden, *downs[:2])
    theirs, own = kernel_call(
        late_kernel,
        (out, out),
        5,
        scratch=half,
        flops=2**29,
        input_output_aliases={4: 0, 5: 1},
    )(where, hidden, *downs[2:], theirs, own)
    return over_tp(where, theirs, own, residual)


def solution(mesh):
    torus = Mesh(
        mesh.devices.reshape(REP, Z, Y, X, CORE), ("rep", "z", "y", "x", "core")
    )
    rep_fs = ("rep", "z", "y")
    tp = ("x", "core")
    in_specs = (P(rep_fs, None), P(), P(("z", "y"), tp), P(tp, ("z", "y")))
    return jax.shard_map(
        shards,
        mesh=torus,
        in_specs=in_specs,
        out_specs=P(rep_fs + tp, None),
        check_vma=False,
    )
```

```python
import jax
import jax.numpy as jnp
from jax import lax
from jax.experimental import pallas as pl
from jax.experimental.pallas import tpu as pltpu
from jax.sharding import Mesh
from jax.sharding import PartitionSpec as P


EPS = 1e-06
REP, Z, Y, X, CORE = 2, 8, 8, 4, 2
VMEM = pl.BlockSpec(memory_space=pltpu.VMEM)
SMEM = pl.BlockSpec(memory_space=pltpu.SMEM)


UP_STEPS = (("y", 4), ("z", 4), ("y", 2), ("z", 2), ("z", 1), ("y", 1))
DOWN_STEPS = (("z", 4), ("y", 4), ("z", 2), ("y", 2), ("y", 1), ("z", 1))


def from_side(array, axis, shift):
    names, size = (("y", "core"), Y) if axis == "y" else (("rep", "z", "core"), REP * Z)
    pairs = []
    for i in range(size):
        pairs.append(((i + shift) % size * 2, i * 2))
        pairs.append(((i - shift) % size * 2 + 1, i * 2 + 1))
    return lax.ppermute(array, names, pairs)


def along_x(array, ahead):
    pairs = [(x, (x + ahead) % X) for x in range(X)]
    return lax.ppermute(array, "x", pairs)


def offsets(steps):
    laid = [(0, 0)]
    for axis, shift in steps:
        dz, dy = (shift, 0) if axis == "z" else (0, shift)
        laid = laid + [(z + dz, y + dy) for z, y in laid]
    return laid


def kernel_call(kernel, outs, n_vmem, scratch=(), smem=True, mib=8, flops=0, **rest):
    single = not isinstance(outs, tuple)
    return pl.pallas_call(
        kernel,
        out_shape=outs,
        in_specs=([SMEM] if smem else []) + [VMEM] * n_vmem,
        out_specs=VMEM if single else (VMEM,) * len(outs),
        scratch_shapes=[pltpu.VMEM(s, jnp.bfloat16) for s in scratch],
        compiler_params=pltpu.CompilerParams(vmem_limit_bytes=mib * 2**20),
        cost_estimate=pl.CostEstimate(
            flops=flops, bytes_accessed=2**20, transcendentals=0
        )
        if flops
        else None,
        **rest,
    )


def bf16(*shape):
    return jax.ShapeDtypeStruct(shape, jnp.bfloat16)


def join_kernel(a, b, out):
    n = a.shape[0]
    out[:n] = a[...]
    out[n:] = b[...]


def join(a, b):
    n = a.shape[0]
    return kernel_call(join_kernel, bf16(2 * n, 32, 512), 2, smem=False)(a, b)


def stage_kernel(where, up, down, up_out, down_out):
    up_out[...] = up[...]
    down_out[...] = down[...]


def norm_kernel(tokens, gain, normed):
    @pl.loop(0, 16)
    def _(n):
        rows = pl.ds(pl.multiple_of(n * 32, 32), 32)
        xf = tokens[rows, :].astype(jnp.float32)
        scale = lax.rsqrt(jnp.mean(xf * xf, axis=-1, keepdims=True) + EPS)
        normed[rows, :] = (xf * scale * gain[...]).astype(jnp.bfloat16)


def place(where, piece, laid, whole, halved):
    z, y, sign = where[0], where[1], 1 - 2 * where[2]
    for j, (dz, dy) in enumerate(laid):
        at_z = (z + sign * dz) & (Z - 1)
        at_y = (y + sign * dy) & (Y - 1)
        at = ((at_z >> 1) if halved else at_z) * Y + at_y
        whole[pl.ds(pl.multiple_of(at * 32, 32), 32), :] = piece[j]


def down_product(hidden, rows, down, out, part):
    @pl.loop(0, 4)
    def _(n):
        columns = pl.ds(pl.multiple_of(n * 256, 256), 256)
        out[part, :, columns] = lax.dot_general(
            hidden[rows, :],
            down[columns, :],
            (((1,), (1,)), ((), ())),
            preferred_element_type=jnp.float32,
        ).astype(jnp.bfloat16)


THEIRS, OWN = slice(0, 256), slice(256, 512)


def up_kernel(where, normed, u0, u1, hidden, up):
    laid = offsets(UP_STEPS)
    place(where, u0, laid[:32], up, False)
    place(where, u1, laid[32:], up, False)
    core = where[2]

    @pl.loop(0, 2)
    def _(n):
        columns = pl.ds(pl.multiple_of(n * 256, 256), 256)
        lifted = jnp.dot(
            normed[...], up[:, columns], preferred_element_type=jnp.float32
        )
        active = jnp.square(jnp.maximum(lifted, 0.0)).astype(jnp.bfloat16)
        for j in range(X * CORE):
            x, c = divmod(j, CORE)
            side = jnp.where(core == c, 256, 0)
            rows = pl.ds(pl.multiple_of(side + x * 64, 64), 64)
            hidden[rows, columns] = active[j * 64 : (j + 1) * 64]


def early_kernel(where, hidden, d0, theirs, own, down):
    place(where, d0, offsets(DOWN_STEPS)[:32], down, True)
    down_product(hidden, THEIRS, down, theirs, 0)
    down_product(hidden, OWN, down, own, 0)


def late_kernel(where, hidden, d1, theirs_in, theirs, down):
    place(where, d1, offsets(DOWN_STEPS)[32:], down, True)
    down_product(hidden, THEIRS, down, theirs, 1)


def own_kernel(hidden, down, own_in, own):
    down_product(hidden, OWN, down, own, 1)


def add_kernel(where, own, beside, keep, ahead, back, far):
    x = where[3]
    for out, step in ((far, 2), (ahead, 1), (back, 3), (keep, 0)):
        rows = pl.ds(pl.multiple_of(((x + step) & (X - 1)) * 64, 64), 64)
        for part in range(2):
            total = own[part, rows].astype(jnp.float32)
            total = total + beside[part, rows].astype(jnp.float32)
            out[part] = total.astype(jnp.bfloat16)


def last_kernel(where, residual, a, b, c, d, out):
    odd = where[0] & 1
    for part in range(2):
        for k in range(4):
            at = (2 * k + (odd ^ part)) * 256
            columns = pl.ds(pl.multiple_of(at, 256), 256)
            here = slice(k * 256, (k + 1) * 256)
            total = residual[:, columns].astype(jnp.float32)
            for term in (a, b, c, d):
                total = total + term[part, :, here].astype(jnp.float32)
            out[:, columns] = total.astype(jnp.bfloat16)


def gathered(where, up, down):
    for k in range(5):
        up_in = from_side(up, *UP_STEPS[k])
        down_in = from_side(down, *DOWN_STEPS[k])
        if k == 0:
            own = bf16(1, 32, 512)
            up, down = kernel_call(stage_kernel, (own, own), 2)(where, up, down)
        up = join(up, up_in)
        down = join(down, down_in)
    up_in = from_side(up, *UP_STEPS[5])
    down_in = from_side(down, *DOWN_STEPS[5])
    return (up, up_in), (down, down_in)


def over_tp(where, beside, own, residual):
    piece = bf16(2, 64, 1024)
    keep, ahead, back, far = kernel_call(add_kernel, (piece,) * 4, 2)(
        where, own, beside
    )
    far, ahead, back = along_x(far, 2), along_x(ahead, 1), along_x(back, 3)
    return kernel_call(last_kernel, bf16(64, 2048), 5)(
        where, residual, keep, ahead, back, far
    )


def shards(tokens, norm_gain, up_weight, down_weight):
    core, x = lax.axis_index("core"), lax.axis_index("x")
    where = jnp.stack([lax.axis_index("z"), lax.axis_index("y"), core, x]).astype(
        jnp.int32
    )
    up, down = gathered(where, up_weight[None], down_weight.T[None])
    normed = kernel_call(
        norm_kernel, bf16(512, 2048), 2, smem=False, mib=12, flops=2**24
    )(tokens, norm_gain[None])
    residual = lax.dynamic_slice_in_dim(tokens, (x * CORE + core) * 64, 64, 0)
    hidden = kernel_call(
        up_kernel, bf16(512, 512), 3, scratch=((2048, 512),), mib=12, flops=2**30
    )(where, normed, *up)
    out = bf16(2, 256, 1024)
    theirs, own = kernel_call(
        early_kernel, (out, out), 2, scratch=((1024, 512),), flops=2**29
    )(where, hidden, down[0])
    theirs, rest = kernel_call(
        late_kernel,
        (out, bf16(1024, 512)),
        3,
        flops=2**28,
        input_output_aliases={3: 0},
    )(where, hidden, down[1], theirs)
    beside = lax.ppermute(theirs, "core", [(0, 1), (1, 0)])
    own = kernel_call(
        own_kernel,
        out,
        3,
        smem=False,
        flops=2**28,
        input_output_aliases={2: 0},
    )(hidden, rest, own)
    return over_tp(where, beside, own, residual)


def solution(mesh):
    torus = Mesh(
        mesh.devices.reshape(REP, Z, Y, X, CORE), ("rep", "z", "y", "x", "core")
    )
    rep_fs = ("rep", "z", "y")
    tp = ("x", "core")
    in_specs = (P(rep_fs, None), P(), P(("z", "y"), tp), P(tp, ("z", "y")))
    return jax.shard_map(
        shards,
        mesh=torus,
        in_specs=in_specs,
        out_specs=P(rep_fs + tp, None),
        check_vma=False,
    )
```

```python
import jax
import jax.numpy as jnp
from jax import lax
from jax.experimental import pallas as pl
from jax.experimental.pallas import tpu as pltpu
from jax.sharding import Mesh
from jax.sharding import PartitionSpec as P


EPS = 1e-06
REP, Z, Y, X, CORE = 2, 8, 8, 4, 2
VMEM = pl.BlockSpec(memory_space=pltpu.VMEM)
SMEM = pl.BlockSpec(memory_space=pltpu.SMEM)


UP_STEPS = (("y", 4), ("z", 4), ("y", 2), ("z", 2))
DOWN_STEPS = (("z", 4), ("y", 4), ("z", 2), ("y", 2))


def from_side(array, axis, shift):
    names, size = (("y", "core"), Y) if axis == "y" else (("rep", "z", "core"), REP * Z)
    pairs = []
    for i in range(size):
        pairs.append(((i + shift) % size * 2, i * 2))
        pairs.append(((i - shift) % size * 2 + 1, i * 2 + 1))
    return lax.ppermute(array, names, pairs)


def between_x(array, first, second):
    pairs = []
    for x in range(X):
        pairs.append((x * 2, (x ^ first) * 2))
        pairs.append((x * 2 + 1, (x ^ second) * 2 + 1))
    return lax.ppermute(array, ("x", "core"), pairs)


def offsets(steps):
    laid = [(0, 0)]
    for axis, shift in steps:
        dz, dy = (shift, 0) if axis == "z" else (0, shift)
        laid = laid + [(z + dz, y + dy) for z, y in laid]
    return laid


def shifted(steps, dz, dy):
    return [(z + dz, y + dy) for z, y in offsets(steps)]


def kernel_call(kernel, outs, n_vmem, scratch=(), smem=True, mib=8, flops=0, **rest):
    single = not isinstance(outs, tuple)
    return pl.pallas_call(
        kernel,
        out_shape=outs,
        in_specs=([SMEM] if smem else []) + [VMEM] * n_vmem,
        out_specs=VMEM if single else (VMEM,) * len(outs),
        scratch_shapes=[pltpu.VMEM(s, jnp.bfloat16) for s in scratch],
        compiler_params=pltpu.CompilerParams(vmem_limit_bytes=mib * 2**20),
        cost_estimate=pl.CostEstimate(
            flops=flops, bytes_accessed=2**20, transcendentals=0
        )
        if flops
        else None,
        **rest,
    )


def bf16(*shape):
    return jax.ShapeDtypeStruct(shape, jnp.bfloat16)


def join_kernel(a, b, out):
    n = a.shape[0]
    out[:n] = a[...]
    out[n:] = b[...]


def join(a, b):
    n = a.shape[0]
    return kernel_call(join_kernel, bf16(2 * n, 32, 512), 2, smem=False)(a, b)


def stage_kernel(where, up, down, up_out, down_out):
    up_out[...] = up[...]
    down_out[...] = down[...]


def norm_kernel(tokens, gain, normed):
    @pl.loop(0, 16)
    def _(n):
        rows = pl.ds(pl.multiple_of(n * 32, 32), 32)
        xf = tokens[rows, :].astype(jnp.float32)
        scale = lax.rsqrt(jnp.mean(xf * xf, axis=-1, keepdims=True) + EPS)
        normed[rows, :] = (xf * scale * gain[...]).astype(jnp.bfloat16)


def place(where, piece, laid, whole, halved):
    z, y, sign = where[0], where[1], 1 - 2 * where[2]
    for j, (dz, dy) in enumerate(laid):
        at_z = (z + sign * dz) & (Z - 1)
        at_y = (y + sign * dy) & (Y - 1)
        at = ((at_z >> 1) if halved else at_z) * Y + at_y
        whole[pl.ds(pl.multiple_of(at * 32, 32), 32), :] = piece[j]


def down_product(hidden, rows, down, out, part):
    @pl.loop(0, 4)
    def _(n):
        columns = pl.ds(pl.multiple_of(n * 256, 256), 256)
        out[part, :, columns] = lax.dot_general(
            hidden[rows, :],
            down[columns, :],
            (((1,), (1,)), ((), ())),
            preferred_element_type=jnp.float32,
        ).astype(jnp.bfloat16)


THEIRS, OWN = slice(0, 256), slice(256, 512)


def up_kernel(where, normed, u0, uz, uy, uzy, hidden, up):
    for piece, shift in ((u0, (0, 0)), (uz, (1, 0)), (uy, (0, 1)), (uzy, (1, 1))):
        place(where, piece, shifted(UP_STEPS, *shift), up, False)
    core = where[2]

    @pl.loop(0, 2)
    def _(n):
        columns = pl.ds(pl.multiple_of(n * 256, 256), 256)
        lifted = jnp.dot(
            normed[...], up[:, columns], preferred_element_type=jnp.float32
        )
        active = jnp.square(jnp.maximum(lifted, 0.0)).astype(jnp.bfloat16)
        for j in range(X * CORE):
            x, c = divmod(j, CORE)
            side = jnp.where(core == c, 256, 0)
            rows = pl.ds(pl.multiple_of(side + x * 64, 64), 64)
            hidden[rows, columns] = active[j * 64 : (j + 1) * 64]


def early_kernel(where, hidden, d0, dy, theirs, own, down):
    place(where, d0, offsets(DOWN_STEPS), down, True)
    place(where, dy, shifted(DOWN_STEPS, 0, 1), down, True)
    down_product(hidden, THEIRS, down, theirs, 0)
    down_product(hidden, OWN, down, own, 0)


def late_kernel(where, hidden, dz, dyz, theirs_in, theirs, down):
    place(where, dz, shifted(DOWN_STEPS, 1, 0), down, True)
    place(where, dyz, shifted(DOWN_STEPS, 1, 1), down, True)
    down_product(hidden, THEIRS, down, theirs, 1)


def own_kernel(hidden, down, own_in, own):
    down_product(hidden, OWN, down, own, 1)


def add_kernel(where, own, beside, keep, send):
    x, core = where[3], where[2]
    first, second = 1 + 2 * core, 3 - 2 * core
    for out, k, chunk in (
        (send, 0, x ^ first),
        (send, 1, x ^ 2),
        (keep, 0, x),
        (keep, 1, x ^ second),
    ):
        rows = pl.ds(pl.multiple_of(chunk * 64, 64), 64)
        for part in range(2):
            total = own[part, rows].astype(jnp.float32)
            total = total + beside[part, rows].astype(jnp.float32)
            out[k, part] = total.astype(jnp.bfloat16)


def pass_kernel(keep, came, out):
    total = keep[1].astype(jnp.float32) + came[1].astype(jnp.float32)
    out[...] = total.astype(jnp.bfloat16)


def last_kernel(where, residual, keep, came, late, out):
    odd = where[0] & 1
    for part in range(2):
        for k in range(4):
            at = (2 * k + (odd ^ part)) * 256
            columns = pl.ds(pl.multiple_of(at, 256), 256)
            here = slice(k * 256, (k + 1) * 256)
            total = residual[:, columns].astype(jnp.float32)
            for term in (keep.at[0], came.at[0], late):
                total = total + term[part, :, here].astype(jnp.float32)
            out[:, columns] = total.astype(jnp.bfloat16)


def gathered(where, up, down):
    for k in range(4):
        up_in = from_side(up, *UP_STEPS[k])
        down_in = from_side(down, *DOWN_STEPS[k])
        if k == 0:
            own = bf16(1, 32, 512)
            up, down = kernel_call(stage_kernel, (own, own), 2)(where, up, down)
        up = join(up, up_in)
        down = join(down, down_in)
    up_z = from_side(up, "z", 1)
    up_y = from_side(up, "y", 1)
    down_y = from_side(down, "y", 1)
    down_z = from_side(down, "z", 1)
    up_zy = from_side(up_z, "y", 1)
    down_yz = from_side(down_y, "z", 1)
    return (up, up_z, up_y, up_zy), (down, down_y, down_z, down_yz)


def over_tp(where, beside, own, residual):
    two = bf16(2, 2, 64, 1024)
    keep, send = kernel_call(add_kernel, (two, two), 2)(where, own, beside)
    came = between_x(send, 1, 3)
    passed = kernel_call(pass_kernel, bf16(2, 64, 1024), 2, smem=False)(keep, came)
    late = between_x(passed, 3, 1)
    return kernel_call(last_kernel, bf16(64, 2048), 4)(
        where, residual, keep, came, late
    )


def shards(tokens, norm_gain, up_weight, down_weight):
    core, x = lax.axis_index("core"), lax.axis_index("x")
    where = jnp.stack([lax.axis_index("z"), lax.axis_index("y"), core, x]).astype(
        jnp.int32
    )
    up, down = gathered(where, up_weight[None], down_weight.T[None])
    normed = kernel_call(
        norm_kernel, bf16(512, 2048), 2, smem=False, mib=12, flops=2**24
    )(tokens, norm_gain[None])
    residual = lax.dynamic_slice_in_dim(tokens, (x * CORE + core) * 64, 64, 0)
    hidden = kernel_call(
        up_kernel, bf16(512, 512), 5, scratch=((2048, 512),), mib=12, flops=2**30
    )(where, normed, *up)
    out = bf16(2, 256, 1024)
    theirs, own = kernel_call(
        early_kernel, (out, out), 3, scratch=((1024, 512),), flops=2**29
    )(where, hidden, *down[:2])
    theirs, rest = kernel_call(
        late_kernel,
        (out, bf16(1024, 512)),
        4,
        flops=2**28,
        input_output_aliases={4: 0},
    )(where, hidden, *down[2:], theirs)
    beside = lax.ppermute(theirs, "core", [(0, 1), (1, 0)])
    own = kernel_call(
        own_kernel,
        out,
        3,
        smem=False,
        flops=2**28,
        input_output_aliases={2: 0},
    )(hidden, rest, own)
    return over_tp(where, beside, own, residual)


def solution(mesh):
    torus = Mesh(
        mesh.devices.reshape(REP, Z, Y, X, CORE), ("rep", "z", "y", "x", "core")
    )
    rep_fs = ("rep", "z", "y")
    tp = ("x", "core")
    in_specs = (P(rep_fs, None), P(), P(("z", "y"), tp), P(tp, ("z", "y")))
    return jax.shard_map(
        shards,
        mesh=torus,
        in_specs=in_specs,
        out_specs=P(rep_fs + tp, None),
        check_vma=False,
    )
```

```python
import jax
import jax.numpy as jnp
from jax import lax
from jax.experimental import pallas as pl
from jax.experimental.pallas import tpu as pltpu
from jax.sharding import Mesh
from jax.sharding import PartitionSpec as P


EPS = 1e-06
REP, Z, Y, X, CORE = 2, 8, 8, 4, 2
VMEM = pl.BlockSpec(memory_space=pltpu.VMEM)
SMEM = pl.BlockSpec(memory_space=pltpu.SMEM)


UP_STEPS = (("y", 4), ("z", 4), ("y", 2), ("z", 2))
DOWN_STEPS = (("z", 4), ("y", 4), ("z", 2), ("y", 2))


def from_side(array, axis, shift):
    names, size = (("y", "core"), Y) if axis == "y" else (("rep", "z", "core"), REP * Z)
    pairs = []
    for i in range(size):
        pairs.append(((i + shift) % size * 2, i * 2))
        pairs.append(((i - shift) % size * 2 + 1, i * 2 + 1))
    return lax.ppermute(array, names, pairs)


def between_x(array, first, second):
    pairs = []
    for x in range(X):
        pairs.append((x * 2, (x ^ first) * 2))
        pairs.append((x * 2 + 1, (x ^ second) * 2 + 1))
    return lax.ppermute(array, ("x", "core"), pairs)


def offsets(steps):
    laid = [(0, 0)]
    for axis, shift in steps:
        dz, dy = (shift, 0) if axis == "z" else (0, shift)
        laid = laid + [(z + dz, y + dy) for z, y in laid]
    return laid


def shifted(steps, dz, dy):
    return [(z + dz, y + dy) for z, y in offsets(steps)]


def kernel_call(kernel, outs, n_vmem, scratch=(), smem=True, mib=8, flops=0, **rest):
    single = not isinstance(outs, tuple)
    return pl.pallas_call(
        kernel,
        out_shape=outs,
        in_specs=([SMEM] if smem else []) + [VMEM] * n_vmem,
        out_specs=VMEM if single else (VMEM,) * len(outs),
        scratch_shapes=[pltpu.VMEM(s, jnp.bfloat16) for s in scratch],
        compiler_params=pltpu.CompilerParams(vmem_limit_bytes=mib * 2**20),
        cost_estimate=pl.CostEstimate(
            flops=flops, bytes_accessed=2**20, transcendentals=0
        )
        if flops
        else None,
        **rest,
    )


def bf16(*shape):
    return jax.ShapeDtypeStruct(shape, jnp.bfloat16)


def join_kernel(a, b, out):
    n = a.shape[0]
    out[:n] = a[...]
    out[n:] = b[...]


def join(a, b):
    n = a.shape[0]
    return kernel_call(join_kernel, bf16(2 * n, 32, 512), 2, smem=False)(a, b)


def stage_kernel(where, up, down, up_out, down_out):
    up_out[...] = up[...]
    down_out[...] = down[...]


def norm_kernel(where, tokens, gain, normed, residual):
    mine = where[3] * CORE + where[2]
    residual[...] = tokens[pl.ds(pl.multiple_of(mine * 64, 64), 64), :]

    @pl.loop(0, 16)
    def _(n):
        rows = pl.ds(pl.multiple_of(n * 32, 32), 32)
        xf = tokens[rows, :].astype(jnp.float32)
        scale = lax.rsqrt(jnp.mean(xf * xf, axis=-1, keepdims=True) + EPS)
        normed[rows, :] = (xf * scale * gain[...]).astype(jnp.bfloat16)


def place(where, piece, laid, whole, halved):
    z, y, sign = where[0], where[1], 1 - 2 * where[2]
    for j, (dz, dy) in enumerate(laid):
        at_z = (z + sign * dz) & (Z - 1)
        at_y = (y + sign * dy) & (Y - 1)
        at = ((at_z >> 1) if halved else at_z) * Y + at_y
        whole[pl.ds(pl.multiple_of(at * 32, 32), 32), :] = piece[j]


def down_product(hidden, rows, down, out, part):
    @pl.loop(0, 4)
    def _(n):
        columns = pl.ds(pl.multiple_of(n * 256, 256), 256)
        out[part, :, columns] = lax.dot_general(
            hidden[rows, :],
            down[columns, :],
            (((1,), (1,)), ((), ())),
            preferred_element_type=jnp.float32,
        ).astype(jnp.bfloat16)


THEIRS, OWN = slice(0, 256), slice(256, 512)


def up_kernel(where, normed, u0, uz, uy, uzy, hidden, up):
    for piece, shift in ((u0, (0, 0)), (uz, (1, 0)), (uy, (0, 1)), (uzy, (1, 1))):
        place(where, piece, shifted(UP_STEPS, *shift), up, False)
    core = where[2]

    @pl.loop(0, 2)
    def _(n):
        columns = pl.ds(pl.multiple_of(n * 256, 256), 256)
        lifted = jnp.dot(
            normed[...], up[:, columns], preferred_element_type=jnp.float32
        )
        active = jnp.square(jnp.maximum(lifted, 0.0)).astype(jnp.bfloat16)
        for j in range(X * CORE):
            x, c = divmod(j, CORE)
            side = jnp.where(core == c, 256, 0)
            rows = pl.ds(pl.multiple_of(side + x * 64, 64), 64)
            hidden[rows, columns] = active[j * 64 : (j + 1) * 64]


def early_kernel(where, hidden, d0, dy, theirs, down):
    place(where, d0, offsets(DOWN_STEPS), down, True)
    place(where, dy, shifted(DOWN_STEPS, 0, 1), down, True)
    down_product(hidden, THEIRS, down, theirs, 0)


def late_kernel(where, hidden, dz, dyz, theirs_in, theirs, down):
    place(where, dz, shifted(DOWN_STEPS, 1, 0), down, True)
    place(where, dyz, shifted(DOWN_STEPS, 1, 1), down, True)
    down_product(hidden, THEIRS, down, theirs, 1)


def own_kernel(hidden, first, second, own):
    down_product(hidden, OWN, first, own, 0)
    down_product(hidden, OWN, second, own, 1)


def add_kernel(where, own, beside, keep, send):
    x, core = where[3], where[2]
    first, second = 1 + 2 * core, 3 - 2 * core
    for out, k, chunk in (
        (send, 0, x ^ first),
        (send, 1, x ^ 2),
        (keep, 0, x),
        (keep, 1, x ^ second),
    ):
        rows = pl.ds(pl.multiple_of(chunk * 64, 64), 64)
        for part in range(2):
            total = own[part, rows].astype(jnp.float32)
            total = total + beside[part, rows].astype(jnp.float32)
            out[k, part] = total.astype(jnp.bfloat16)


def pass_kernel(keep, came, out):
    total = keep[1].astype(jnp.float32) + came[1].astype(jnp.float32)
    out[...] = total.astype(jnp.bfloat16)


def last_kernel(where, residual, keep, came, late, out):
    odd = where[0] & 1
    for part in range(2):
        for k in range(4):
            at = (2 * k + (odd ^ part)) * 256
            columns = pl.ds(pl.multiple_of(at, 256), 256)
            here = slice(k * 256, (k + 1) * 256)
            total = residual[:, columns].astype(jnp.float32)
            for term in (keep.at[0], came.at[0], late):
                total = total + term[part, :, here].astype(jnp.float32)
            out[:, columns] = total.astype(jnp.bfloat16)


def gathered(where, up, down):
    for k in range(4):
        up_in = from_side(up, *UP_STEPS[k])
        down_in = from_side(down, *DOWN_STEPS[k])
        if k == 0:
            own = bf16(1, 32, 512)
            up, down = kernel_call(stage_kernel, (own, own), 2)(where, up, down)
        up = join(up, up_in)
        down = join(down, down_in)
    up_z = from_side(up, "z", 1)
    up_y = from_side(up, "y", 1)
    down_y = from_side(down, "y", 1)
    down_z = from_side(down, "z", 1)
    up_zy = from_side(up_z, "y", 1)
    down_yz = from_side(down_y, "z", 1)
    return (up, up_z, up_y, up_zy), (down, down_y, down_z, down_yz)


def over_tp(where, beside, own, residual):
    two = bf16(2, 2, 64, 1024)
    keep, send = kernel_call(add_kernel, (two, two), 2)(where, own, beside)
    came = between_x(send, 1, 3)
    passed = kernel_call(pass_kernel, bf16(2, 64, 1024), 2, smem=False)(keep, came)
    late = between_x(passed, 3, 1)
    return kernel_call(last_kernel, bf16(64, 2048), 4)(
        where, residual, keep, came, late
    )


def shards(tokens, norm_gain, up_weight, down_weight):
    core, x = lax.axis_index("core"), lax.axis_index("x")
    where = jnp.stack([lax.axis_index("z"), lax.axis_index("y"), core, x]).astype(
        jnp.int32
    )
    up, down = gathered(where, up_weight[None], down_weight.T[None])
    normed, residual = kernel_call(
        norm_kernel, (bf16(512, 2048), bf16(64, 2048)), 2, mib=12, flops=2**24
    )(where, tokens, norm_gain[None])
    hidden = kernel_call(
        up_kernel, bf16(512, 512), 5, scratch=((2048, 512),), mib=12, flops=2**30
    )(where, normed, *up)
    out = bf16(2, 256, 1024)
    theirs, first = kernel_call(
        early_kernel, (out, bf16(1024, 512)), 3, flops=2**28
    )(where, hidden, *down[:2])
    theirs, second = kernel_call(
        late_kernel,
        (out, bf16(1024, 512)),
        4,
        flops=2**28,
        input_output_aliases={4: 0},
    )(where, hidden, *down[2:], theirs)
    beside = lax.ppermute(theirs, "core", [(0, 1), (1, 0)])
    own = kernel_call(own_kernel, out, 3, smem=False, flops=2**29)(
        hidden, first, second
    )
    return over_tp(where, beside, own, residual)


def solution(mesh):
    torus = Mesh(
        mesh.devices.reshape(REP, Z, Y, X, CORE), ("rep", "z", "y", "x", "core")
    )
    rep_fs = ("rep", "z", "y")
    tp = ("x", "core")
    in_specs = (P(rep_fs, None), P(), P(("z", "y"), tp), P(tp, ("z", "y")))
    return jax.shard_map(
        shards,
        mesh=torus,
        in_specs=in_specs,
        out_specs=P(rep_fs + tp, None),
        check_vma=False,
    )
```

```python
import jax
import jax.numpy as jnp
from jax import lax
from jax.experimental import pallas as pl
from jax.experimental.pallas import tpu as pltpu
from jax.sharding import Mesh
from jax.sharding import PartitionSpec as P


EPS = 1e-06
REP, Z, Y, X, CORE = 2, 8, 8, 4, 2
VMEM = pl.BlockSpec(memory_space=pltpu.VMEM)


UP_STEPS = (("y", 4), ("z", 4), ("y", 2), ("z", 2))
DOWN_STEPS = (("z", 4), ("y", 4), ("z", 2), ("y", 2))


def from_side(array, axis, shift):
    names, size = (("y", "core"), Y) if axis == "y" else (("rep", "z", "core"), REP * Z)
    pairs = []
    for i in range(size):
        pairs.append(((i + shift) % size * 2, i * 2))
        pairs.append(((i - shift) % size * 2 + 1, i * 2 + 1))
    return lax.ppermute(array, names, pairs)


def between_x(array, first, second):
    pairs = []
    for x in range(X):
        pairs.append((x * 2, (x ^ first) * 2))
        pairs.append((x * 2 + 1, (x ^ second) * 2 + 1))
    return lax.ppermute(array, ("x", "core"), pairs)


def offsets(steps):
    laid = [(0, 0)]
    for axis, shift in steps:
        dz, dy = (shift, 0) if axis == "z" else (0, shift)
        laid = laid + [(z + dz, y + dy) for z, y in laid]
    return laid


def shifted(steps, dz, dy):
    return [(z + dz, y + dy) for z, y in offsets(steps)]


def kernel_call(kernel, outs, n_vmem, scratch=(), mib=8, flops=0, **rest):
    single = not isinstance(outs, tuple)
    return pl.pallas_call(
        kernel,
        out_shape=outs,
        in_specs=[VMEM] * n_vmem,
        out_specs=VMEM if single else (VMEM,) * len(outs),
        scratch_shapes=[pltpu.VMEM(s, jnp.bfloat16) for s in scratch],
        compiler_params=pltpu.CompilerParams(vmem_limit_bytes=mib * 2**20),
        cost_estimate=pl.CostEstimate(
            flops=flops, bytes_accessed=2**20, transcendentals=0
        )
        if flops
        else None,
        **rest,
    )


def bf16(*shape):
    return jax.ShapeDtypeStruct(shape, jnp.bfloat16)


def join_kernel(a, b, out):
    n = a.shape[0]
    out[:n] = a[...]
    out[n:] = b[...]


def join(a, b):
    n = a.shape[0]
    return kernel_call(join_kernel, bf16(2 * n, 32, 512), 2)(a, b)


def stage_kernel(up, down, up_out, down_out):
    up_out[...] = up[...]
    down_out[...] = down[...]


def norm_kernel(tokens, gain, normed, residual):
    mine = lax.axis_index("x") * CORE + lax.axis_index("core")
    residual[...] = tokens[pl.ds(pl.multiple_of(mine * 64, 64), 64), :]

    @pl.loop(0, 16)
    def _(n):
        rows = pl.ds(pl.multiple_of(n * 32, 32), 32)
        xf = tokens[rows, :].astype(jnp.float32)
        scale = lax.rsqrt(jnp.mean(xf * xf, axis=-1, keepdims=True) + EPS)
        normed[rows, :] = (xf * scale * gain[...]).astype(jnp.bfloat16)


def place(piece, laid, whole, halved):
    z, y = lax.axis_index("z"), lax.axis_index("y")
    sign = 1 - 2 * lax.axis_index("core")
    for j, (dz, dy) in enumerate(laid):
        at_z = (z + sign * dz) & (Z - 1)
        at_y = (y + sign * dy) & (Y - 1)
        at = ((at_z >> 1) if halved else at_z) * Y + at_y
        whole[pl.ds(pl.multiple_of(at * 32, 32), 32), :] = piece[j]


def down_product(hidden, rows, down, out):
    @pl.loop(0, 4)
    def _(n):
        columns = pl.ds(pl.multiple_of(n * 256, 256), 256)
        out[:, columns] = lax.dot_general(
            hidden[rows, :],
            down[columns, :],
            (((1,), (1,)), ((), ())),
            preferred_element_type=jnp.float32,
        ).astype(jnp.bfloat16)


THEIRS, OWN = slice(0, 256), slice(256, 512)


def up_kernel(normed, u0, uz, uy, uzy, hidden, up):
    for piece, shift in ((u0, (0, 0)), (uz, (1, 0)), (uy, (0, 1)), (uzy, (1, 1))):
        place(piece, shifted(UP_STEPS, *shift), up, False)
    core = lax.axis_index("core")

    @pl.loop(0, 2)
    def _(n):
        columns = pl.ds(pl.multiple_of(n * 256, 256), 256)
        lifted = jnp.dot(
            normed[...], up[:, columns], preferred_element_type=jnp.float32
        )
        active = jnp.square(jnp.maximum(lifted, 0.0)).astype(jnp.bfloat16)
        for j in range(X * CORE):
            x, c = divmod(j, CORE)
            side = jnp.where(core == c, 256, 0)
            rows = pl.ds(pl.multiple_of(side + x * 64, 64), 64)
            hidden[rows, columns] = active[j * 64 : (j + 1) * 64]


def early_kernel(hidden, d0, dy, theirs, down):
    place(d0, offsets(DOWN_STEPS), down, True)
    place(dy, shifted(DOWN_STEPS, 0, 1), down, True)
    down_product(hidden, THEIRS, down, theirs)


def late_kernel(hidden, dz, dyz, theirs, down):
    place(dz, shifted(DOWN_STEPS, 1, 0), down, True)
    place(dyz, shifted(DOWN_STEPS, 1, 1), down, True)
    down_product(hidden, THEIRS, down, theirs)


def own_kernel(hidden, down, own):
    down_product(hidden, OWN, down, own)


def add_kernel(own, beside, keep, send):
    x, core = lax.axis_index("x"), lax.axis_index("core")
    first, second = 1 + 2 * core, 3 - 2 * core
    for out, k, chunk in (
        (send, 0, x ^ first),
        (send, 1, x ^ 2),
        (keep, 0, x),
        (keep, 1, x ^ second),
    ):
        rows = pl.ds(pl.multiple_of(chunk * 64, 64), 64)
        total = own[rows].astype(jnp.float32) + beside[rows].astype(jnp.float32)
        out[k] = total.astype(jnp.bfloat16)


def pass_kernel(keep, came, out):
    total = keep[1].astype(jnp.float32) + came[1].astype(jnp.float32)
    out[...] = total.astype(jnp.bfloat16)


def last_kernel(residual, keep0, came0, late0, keep1, came1, late1, out):
    odd = lax.axis_index("z") & 1
    for part, terms in ((0, (keep0, came0, late0)), (1, (keep1, came1, late1))):
        for k in range(4):
            at = (2 * k + (odd ^ part)) * 256
            columns = pl.ds(pl.multiple_of(at, 256), 256)
            here = slice(k * 256, (k + 1) * 256)
            total = residual[:, columns].astype(jnp.float32)
            keep, came, late = terms
            for term in (keep.at[0], came.at[0], late):
                total = total + term[:, here].astype(jnp.float32)
            out[:, columns] = total.astype(jnp.bfloat16)


def gathered(up, down):
    for k in range(4):
        up_in = from_side(up, *UP_STEPS[k])
        down_in = from_side(down, *DOWN_STEPS[k])
        if k == 0:
            own = bf16(1, 32, 512)
            up, down = kernel_call(stage_kernel, (own, own), 2)(up, down)
        up = join(up, up_in)
        down = join(down, down_in)
    up_z = from_side(up, "z", 1)
    up_y = from_side(up, "y", 1)
    down_y = from_side(down, "y", 1)
    down_z = from_side(down, "z", 1)
    up_zy = from_side(up_z, "y", 1)
    down_yz = from_side(down_y, "z", 1)
    return (up, up_z, up_y, up_zy), (down, down_y, down_z, down_yz)


def over_tp(beside, own):
    two = bf16(2, 64, 1024)
    keep, send = kernel_call(add_kernel, (two, two), 2)(own, beside)
    came = between_x(send, 1, 3)
    passed = kernel_call(pass_kernel, bf16(64, 1024), 2)(keep, came)
    late = between_x(passed, 3, 1)
    return keep, came, late


def shards(tokens, norm_gain, up_weight, down_weight):
    up, down = gathered(up_weight[None], down_weight.T[None])
    normed, residual = kernel_call(
        norm_kernel, (bf16(512, 2048), bf16(64, 2048)), 2, mib=12, flops=2**24
    )(tokens, norm_gain[None])
    hidden = kernel_call(
        up_kernel, bf16(512, 512), 5, scratch=((2048, 512),), mib=12, flops=2**30
    )(normed, *up)
    out, rows = bf16(256, 1024), bf16(1024, 512)
    trades = []
    for part, kernel in ((0, early_kernel), (1, late_kernel)):
        pieces = down[2 * part : 2 * part + 2]
        theirs, placed = kernel_call(kernel, (out, rows), 3, flops=2**28)(
            hidden, *pieces
        )
        beside = lax.ppermute(theirs, "core", [(0, 1), (1, 0)])
        own = kernel_call(own_kernel, out, 2, flops=2**28)(hidden, placed)
        trades += over_tp(beside, own)
    return kernel_call(last_kernel, bf16(64, 2048), 7)(residual, *trades)


def solution(mesh):
    torus = Mesh(
        mesh.devices.reshape(REP, Z, Y, X, CORE), ("rep", "z", "y", "x", "core")
    )
    rep_fs = ("rep", "z", "y")
    tp = ("x", "core")
    in_specs = (P(rep_fs, None), P(), P(("z", "y"), tp), P(tp, ("z", "y")))
    return jax.shard_map(
        shards,
        mesh=torus,
        in_specs=in_specs,
        out_specs=P(rep_fs + tp, None),
        check_vma=False,
    )
```

```python
import jax
import jax.numpy as jnp
from jax import lax
from jax.experimental import pallas as pl
from jax.experimental.pallas import tpu as pltpu
from jax.sharding import Mesh
from jax.sharding import PartitionSpec as P


EPS = 1e-06
REP, Z, Y, X, CORE = 2, 8, 8, 4, 2
VMEM = pl.BlockSpec(memory_space=pltpu.VMEM)


UP_STEPS = (("y", 4), ("z", 4), ("y", 2), ("z", 2))
DOWN_STEPS = (("z", 4), ("y", 4), ("z", 2), ("y", 2))


def from_side(array, axis, shift):
    names, size = (("y", "core"), Y) if axis == "y" else (("rep", "z", "core"), REP * Z)
    pairs = []
    for i in range(size):
        pairs.append(((i + shift) % size * 2, i * 2))
        pairs.append(((i - shift) % size * 2 + 1, i * 2 + 1))
    return lax.ppermute(array, names, pairs)


def between_x(array, first, second):
    pairs = []
    for x in range(X):
        pairs.append((x * 2, (x ^ first) * 2))
        pairs.append((x * 2 + 1, (x ^ second) * 2 + 1))
    return lax.ppermute(array, ("x", "core"), pairs)


def offsets(steps):
    laid = [(0, 0)]
    for axis, shift in steps:
        dz, dy = (shift, 0) if axis == "z" else (0, shift)
        laid = laid + [(z + dz, y + dy) for z, y in laid]
    return laid


def shifted(steps, dz, dy):
    return [(z + dz, y + dy) for z, y in offsets(steps)]


def kernel_call(kernel, outs, n_vmem, scratch=(), mib=8, flops=0, **rest):
    single = not isinstance(outs, tuple)
    return pl.pallas_call(
        kernel,
        out_shape=outs,
        in_specs=[VMEM] * n_vmem,
        out_specs=VMEM if single else (VMEM,) * len(outs),
        scratch_shapes=[pltpu.VMEM(s, jnp.bfloat16) for s in scratch],
        compiler_params=pltpu.CompilerParams(vmem_limit_bytes=mib * 2**20),
        cost_estimate=pl.CostEstimate(
            flops=flops, bytes_accessed=2**20, transcendentals=0
        )
        if flops
        else None,
        **rest,
    )


def bf16(*shape):
    return jax.ShapeDtypeStruct(shape, jnp.bfloat16)


def join_kernel(a, b, out):
    n = a.shape[0]
    out[:n] = a[...]
    out[n:] = b[...]


def join(a, b):
    n = a.shape[0]
    return kernel_call(join_kernel, bf16(2 * n, 32, 512), 2)(a, b)


def stage_kernel(up, down, up_out, down_out):
    up_out[...] = up[...]
    down_out[...] = down[...]


def norm_kernel(tokens, gain, normed, residual):
    mine = lax.axis_index("x") * CORE + lax.axis_index("core")
    residual[...] = tokens[pl.ds(pl.multiple_of(mine * 64, 64), 64), :]

    @pl.loop(0, 16)
    def _(n):
        rows = pl.ds(pl.multiple_of(n * 32, 32), 32)
        xf = tokens[rows, :].astype(jnp.float32)
        scale = lax.rsqrt(jnp.mean(xf * xf, axis=-1, keepdims=True) + EPS)
        normed[rows, :] = (xf * scale * gain[...]).astype(jnp.bfloat16)


def place(piece, laid, whole, halved):
    z, y = lax.axis_index("z"), lax.axis_index("y")
    sign = 1 - 2 * lax.axis_index("core")
    for j, (dz, dy) in enumerate(laid):
        at_z = (z + sign * dz) & (Z - 1)
        at_y = (y + sign * dy) & (Y - 1)
        at = ((at_z >> 1) if halved else at_z) * Y + at_y
        whole[pl.ds(pl.multiple_of(at * 32, 32), 32), :] = piece[j]


def down_product(hidden, rows, down, out, part):
    @pl.loop(0, 4)
    def _(n):
        columns = pl.ds(pl.multiple_of(n * 256, 256), 256)
        out[part, :, columns] = lax.dot_general(
            hidden[rows, :],
            down[columns, :],
            (((1,), (1,)), ((), ())),
            preferred_element_type=jnp.float32,
        ).astype(jnp.bfloat16)


THEIRS, OWN = slice(0, 256), slice(256, 512)


def up_kernel(normed, u0, uz, uy, uzy, hidden, up):
    for piece, shift in ((u0, (0, 0)), (uz, (1, 0)), (uy, (0, 1)), (uzy, (1, 1))):
        place(piece, shifted(UP_STEPS, *shift), up, False)
    core = lax.axis_index("core")

    @pl.loop(0, 2)
    def _(n):
        columns = pl.ds(pl.multiple_of(n * 256, 256), 256)
        lifted = jnp.dot(
            normed[...], up[:, columns], preferred_element_type=jnp.float32
        )
        active = jnp.square(jnp.maximum(lifted, 0.0)).astype(jnp.bfloat16)
        for j in range(X * CORE):
            x, c = divmod(j, CORE)
            side = jnp.where(core == c, 256, 0)
            rows = pl.ds(pl.multiple_of(side + x * 64, 64), 64)
            hidden[rows, columns] = active[j * 64 : (j + 1) * 64]


def early_kernel(hidden, d0, dy, theirs, down):
    place(d0, offsets(DOWN_STEPS), down, True)
    place(dy, shifted(DOWN_STEPS, 0, 1), down, True)
    down_product(hidden, THEIRS, down, theirs, 0)


def late_kernel(hidden, dz, dyz, theirs_in, theirs, down):
    place(dz, shifted(DOWN_STEPS, 1, 0), down, True)
    place(dyz, shifted(DOWN_STEPS, 1, 1), down, True)
    down_product(hidden, THEIRS, down, theirs, 1)


def own_kernel(hidden, first, second, own):
    down_product(hidden, OWN, first, own, 0)
    down_product(hidden, OWN, second, own, 1)


def add_kernel(own, beside, keep, send):
    x, core = lax.axis_index("x"), lax.axis_index("core")
    first, second = 1 + 2 * core, 3 - 2 * core
    for out, k, chunk in (
        (send, 0, x ^ first),
        (send, 1, x ^ 2),
        (keep, 0, x),
        (keep, 1, x ^ second),
    ):
        rows = pl.ds(pl.multiple_of(chunk * 64, 64), 64)
        for part in range(2):
            total = own[part, rows].astype(jnp.float32)
            total = total + beside[part, rows].astype(jnp.float32)
            out[k, part] = total.astype(jnp.bfloat16)


def pass_kernel(keep, came, out):
    total = keep[1].astype(jnp.float32) + came[1].astype(jnp.float32)
    out[...] = total.astype(jnp.bfloat16)


def last_kernel(residual, keep, came, late, out):
    odd = lax.axis_index("z") & 1
    for part in range(2):
        for k in range(4):
            at = (2 * k + (odd ^ part)) * 256
            columns = pl.ds(pl.multiple_of(at, 256), 256)
            here = slice(k * 256, (k + 1) * 256)
            total = residual[:, columns].astype(jnp.float32)
            for term in (keep.at[0], came.at[0], late):
                total = total + term[part, :, here].astype(jnp.float32)
            out[:, columns] = total.astype(jnp.bfloat16)


def gathered(up, down):
    for k in range(4):
        up_in = from_side(up, *UP_STEPS[k])
        down_in = from_side(down, *DOWN_STEPS[k])
        if k == 0:
            own = bf16(1, 32, 512)
            up, down = kernel_call(stage_kernel, (own, own), 2)(up, down)
        up = join(up, up_in)
        down = join(down, down_in)
    up_z = from_side(up, "z", 1)
    up_y = from_side(up, "y", 1)
    down_y = from_side(down, "y", 1)
    down_z = from_side(down, "z", 1)
    up_zy = from_side(up_z, "y", 1)
    down_yz = from_side(down_y, "z", 1)
    return (up, up_z, up_y, up_zy), (down, down_y, down_z, down_yz)


def over_tp(beside, own, residual):
    two = bf16(2, 2, 64, 1024)
    keep, send = kernel_call(add_kernel, (two, two), 2)(own, beside)
    came = between_x(send, 1, 3)
    passed = kernel_call(pass_kernel, bf16(2, 64, 1024), 2)(keep, came)
    late = between_x(passed, 3, 1)
    return kernel_call(last_kernel, bf16(64, 2048), 4)(residual, keep, came, late)


def shards(tokens, norm_gain, up_weight, down_weight):
    up, down = gathered(up_weight[None], down_weight.T[None])
    normed, residual = kernel_call(
        norm_kernel, (bf16(512, 2048), bf16(64, 2048)), 2, mib=12, flops=2**24
    )(tokens, norm_gain[None])
    hidden = kernel_call(
        up_kernel, bf16(512, 512), 5, scratch=((2048, 512),), mib=12, flops=2**30
    )(normed, *up)
    out, rows = bf16(2, 256, 1024), bf16(1024, 512)
    theirs, first = kernel_call(early_kernel, (out, rows), 3, flops=2**28)(
        hidden, *down[:2]
    )
    theirs, second = kernel_call(
        late_kernel,
        (out, rows),
        4,
        flops=2**28,
        input_output_aliases={3: 0},
    )(hidden, *down[2:], theirs)
    beside = lax.ppermute(theirs, "core", [(0, 1), (1, 0)])
    own = kernel_call(own_kernel, out, 3, flops=2**29)(hidden, first, second)
    return over_tp(beside, own, residual)


def solution(mesh):
    torus = Mesh(
        mesh.devices.reshape(REP, Z, Y, X, CORE), ("rep", "z", "y", "x", "core")
    )
    rep_fs = ("rep", "z", "y")
    tp = ("x", "core")
    in_specs = (P(rep_fs, None), P(), P(("z", "y"), tp), P(tp, ("z", "y")))
    return jax.shard_map(
        shards,
        mesh=torus,
        in_specs=in_specs,
        out_specs=P(rep_fs + tp, None),
        check_vma=False,
    )
```

```python
import jax
import jax.numpy as jnp
from jax import lax
from jax.experimental import pallas as pl
from jax.experimental.pallas import tpu as pltpu
from jax.sharding import Mesh
from jax.sharding import PartitionSpec as P


EPS = 1e-06
REP, Z, Y, X, CORE = 2, 8, 8, 4, 2
VMEM = pl.BlockSpec(memory_space=pltpu.VMEM)


UP_STEPS = (("y", 4), ("z", 4), ("y", 2), ("z", 2))
DOWN_STEPS = (("z", 4), ("y", 4), ("z", 2), ("y", 2))


def from_side(array, axis, shift):
    names, size = (("y", "core"), Y) if axis == "y" else (("rep", "z", "core"), REP * Z)
    pairs = []
    for i in range(size):
        pairs.append(((i + shift) % size * 2, i * 2))
        pairs.append(((i - shift) % size * 2 + 1, i * 2 + 1))
    return lax.ppermute(array, names, pairs)


def between_x(array, first, second):
    pairs = []
    for x in range(X):
        pairs.append((x * 2, (x ^ first) * 2))
        pairs.append((x * 2 + 1, (x ^ second) * 2 + 1))
    return lax.ppermute(array, ("x", "core"), pairs)


def offsets(steps):
    laid = [(0, 0)]
    for axis, shift in steps:
        dz, dy = (shift, 0) if axis == "z" else (0, shift)
        laid = laid + [(z + dz, y + dy) for z, y in laid]
    return laid


def shifted(steps, dz, dy):
    return [(z + dz, y + dy) for z, y in offsets(steps)]


def kernel_call(kernel, outs, n_vmem, scratch=(), mib=8, flops=0, **rest):
    single = not isinstance(outs, tuple)
    return pl.pallas_call(
        kernel,
        out_shape=outs,
        in_specs=[VMEM] * n_vmem,
        out_specs=VMEM if single else (VMEM,) * len(outs),
        scratch_shapes=[pltpu.VMEM(s, jnp.bfloat16) for s in scratch],
        compiler_params=pltpu.CompilerParams(vmem_limit_bytes=mib * 2**20),
        cost_estimate=pl.CostEstimate(
            flops=flops, bytes_accessed=2**20, transcendentals=0
        )
        if flops
        else None,
        **rest,
    )


def bf16(*shape):
    return jax.ShapeDtypeStruct(shape, jnp.bfloat16)


def join_kernel(a, b, out):
    n = a.shape[0]
    out[:n] = a[...]
    out[n:] = b[...]


def join(a, b):
    n = a.shape[0]
    return kernel_call(join_kernel, bf16(2 * n, 32, 512), 2)(a, b)


def stage_kernel(up, down, up_out, down_out):
    up_out[...] = up[...]
    down_out[...] = down[...]


def norm_kernel(tokens, gain, normed, residual):
    mine = lax.axis_index("x") * CORE + lax.axis_index("core")
    residual[...] = tokens[pl.ds(pl.multiple_of(mine * 64, 64), 64), :]

    @pl.loop(0, 16)
    def _(n):
        rows = pl.ds(pl.multiple_of(n * 32, 32), 32)
        xf = tokens[rows, :].astype(jnp.float32)
        scale = lax.rsqrt(jnp.mean(xf * xf, axis=-1, keepdims=True) + EPS)
        normed[rows, :] = (xf * scale * gain[...]).astype(jnp.bfloat16)


def place(piece, laid, whole, halved):
    z, y = lax.axis_index("z"), lax.axis_index("y")
    sign = 1 - 2 * lax.axis_index("core")
    for j, (dz, dy) in enumerate(laid):
        at_z = (z + sign * dz) & (Z - 1)
        at_y = (y + sign * dy) & (Y - 1)
        at = ((at_z >> 1) if halved else at_z) * Y + at_y
        whole[pl.ds(pl.multiple_of(at * 32, 32), 32), :] = piece[j]


def down_product(hidden, rows, down, out, part):
    @pl.loop(0, 4)
    def _(n):
        columns = pl.ds(pl.multiple_of(n * 256, 256), 256)
        out[part, :, columns] = lax.dot_general(
            hidden[rows, :],
            down[columns, :],
            (((1,), (1,)), ((), ())),
            preferred_element_type=jnp.float32,
        ).astype(jnp.bfloat16)


THEIRS, OWN = slice(0, 256), slice(256, 512)


def up_kernel(normed, u0, uz, uy, uzy, hidden, up):
    for piece, shift in ((u0, (0, 0)), (uz, (1, 0)), (uy, (0, 1)), (uzy, (1, 1))):
        place(piece, shifted(UP_STEPS, *shift), up, False)
    core = lax.axis_index("core")

    @pl.loop(0, 2)
    def _(n):
        columns = pl.ds(pl.multiple_of(n * 256, 256), 256)
        lifted = jnp.dot(
            normed[...], up[:, columns], preferred_element_type=jnp.float32
        )
        active = jnp.square(jnp.maximum(lifted, 0.0)).astype(jnp.bfloat16)
        for j in range(X * CORE):
            x, c = divmod(j, CORE)
            side = jnp.where(core == c, 256, 0)
            rows = pl.ds(pl.multiple_of(side + x * 64, 64), 64)
            hidden[rows, columns] = active[j * 64 : (j + 1) * 64]


def early_kernel(hidden, d0, dy, theirs, down):
    place(d0, offsets(DOWN_STEPS), down, True)
    place(dy, shifted(DOWN_STEPS, 0, 1), down, True)
    down_product(hidden, THEIRS, down, theirs, 0)


def late_kernel(hidden, dz, dyz, theirs_in, theirs, down):
    place(dz, shifted(DOWN_STEPS, 1, 0), down, True)
    place(dyz, shifted(DOWN_STEPS, 1, 1), down, True)
    down_product(hidden, THEIRS, down, theirs, 1)


def own_kernel(hidden, first, second, own):
    down_product(hidden, OWN, first, own, 0)
    down_product(hidden, OWN, second, own, 1)


def add_kernel(own, beside, ahead, near, keep, hold):
    x, core = lax.axis_index("x"), lax.axis_index("core")
    first, second = 1 + 2 * core, 3 - 2 * core
    for out, chunk in (
        (ahead, x ^ 2),
        (near, x ^ first),
        (keep, x),
        (hold, x ^ second),
    ):
        rows = pl.ds(pl.multiple_of(chunk * 64, 64), 64)
        for part in range(2):
            total = own[part, rows].astype(jnp.float32)
            total = total + beside[part, rows].astype(jnp.float32)
            out[part] = total.astype(jnp.bfloat16)


def pass_kernel(hold, came, out):
    total = hold[...].astype(jnp.float32) + came[...].astype(jnp.float32)
    out[...] = total.astype(jnp.bfloat16)


def last_kernel(residual, keep, came, late, out):
    odd = lax.axis_index("z") & 1
    for part in range(2):
        for k in range(4):
            at = (2 * k + (odd ^ part)) * 256
            columns = pl.ds(pl.multiple_of(at, 256), 256)
            here = slice(k * 256, (k + 1) * 256)
            total = residual[:, columns].astype(jnp.float32)
            for term in (keep, came, late):
                total = total + term[part, :, here].astype(jnp.float32)
            out[:, columns] = total.astype(jnp.bfloat16)


def gathered(up, down):
    for k in range(4):
        up_in = from_side(up, *UP_STEPS[k])
        down_in = from_side(down, *DOWN_STEPS[k])
        if k == 0:
            own = bf16(1, 32, 512)
            up, down = kernel_call(stage_kernel, (own, own), 2)(up, down)
        up = join(up, up_in)
        down = join(down, down_in)
    up_z = from_side(up, "z", 1)
    up_y = from_side(up, "y", 1)
    down_y = from_side(down, "y", 1)
    down_z = from_side(down, "z", 1)
    up_zy = from_side(up_z, "y", 1)
    down_yz = from_side(down_y, "z", 1)
    return (up, up_z, up_y, up_zy), (down, down_y, down_z, down_yz)


def over_tp(beside, own, residual):
    piece = bf16(2, 64, 1024)
    ahead, near, keep, hold = kernel_call(add_kernel, (piece,) * 4, 2)(own, beside)
    through = between_x(ahead, 1, 3)
    came = between_x(near, 1, 3)
    passed = kernel_call(pass_kernel, piece, 2)(hold, through)
    late = between_x(passed, 3, 1)
    return kernel_call(last_kernel, bf16(64, 2048), 4)(residual, keep, came, late)


def shards(tokens, norm_gain, up_weight, down_weight):
    up, down = gathered(up_weight[None], down_weight.T[None])
    normed, residual = kernel_call(
        norm_kernel, (bf16(512, 2048), bf16(64, 2048)), 2, mib=12, flops=2**24
    )(tokens, norm_gain[None])
    hidden = kernel_call(
        up_kernel, bf16(512, 512), 5, scratch=((2048, 512),), mib=12, flops=2**30
    )(normed, *up)
    out, rows = bf16(2, 256, 1024), bf16(1024, 512)
    theirs, first = kernel_call(early_kernel, (out, rows), 3, flops=2**28)(
        hidden, *down[:2]
    )
    theirs, second = kernel_call(
        late_kernel,
        (out, rows),
        4,
        flops=2**28,
        input_output_aliases={3: 0},
    )(hidden, *down[2:], theirs)
    beside = lax.ppermute(theirs, "core", [(0, 1), (1, 0)])
    own = kernel_call(own_kernel, out, 3, flops=2**29)(hidden, first, second)
    return over_tp(beside, own, residual)


def solution(mesh):
    torus = Mesh(
        mesh.devices.reshape(REP, Z, Y, X, CORE), ("rep", "z", "y", "x", "core")
    )
    rep_fs = ("rep", "z", "y")
    tp = ("x", "core")
    in_specs = (P(rep_fs, None), P(), P(("z", "y"), tp), P(tp, ("z", "y")))
    return jax.shard_map(
        shards,
        mesh=torus,
        in_specs=in_specs,
        out_specs=P(rep_fs + tp, None),
        check_vma=False,
    )
```

```python
import jax
import jax.numpy as jnp
from jax import lax
from jax.experimental import pallas as pl
from jax.experimental.pallas import tpu as pltpu
from jax.sharding import Mesh
from jax.sharding import PartitionSpec as P


EPS = 1e-06
REP, Z, Y, X, CORE = 2, 8, 8, 4, 2
VMEM = pl.BlockSpec(memory_space=pltpu.VMEM)


UP_STEPS = (("y", 4), ("z", 4), ("y", 2), ("z", 2))
DOWN_STEPS = (("z", 4), ("y", 4), ("z", 2), ("y", 2))


def from_side(array, axis, shift):
    names, size = (("y", "core"), Y) if axis == "y" else (("rep", "z", "core"), REP * Z)
    pairs = []
    for i in range(size):
        pairs.append(((i - shift) % size * 2, i * 2))
        pairs.append(((i + shift) % size * 2 + 1, i * 2 + 1))
    return lax.ppermute(array, names, pairs)


def between_x(array, first, second):
    pairs = []
    for x in range(X):
        pairs.append((x * 2, (x ^ first) * 2))
        pairs.append((x * 2 + 1, (x ^ second) * 2 + 1))
    return lax.ppermute(array, ("x", "core"), pairs)


def offsets(steps):
    laid = [(0, 0)]
    for axis, shift in steps:
        dz, dy = (shift, 0) if axis == "z" else (0, shift)
        laid = laid + [(z + dz, y + dy) for z, y in laid]
    return laid


def shifted(steps, dz, dy):
    return [(z + dz, y + dy) for z, y in offsets(steps)]


def kernel_call(kernel, outs, n_vmem, scratch=(), mib=8, flops=0, **rest):
    single = not isinstance(outs, tuple)
    return pl.pallas_call(
        kernel,
        out_shape=outs,
        in_specs=[VMEM] * n_vmem,
        out_specs=VMEM if single else (VMEM,) * len(outs),
        scratch_shapes=[pltpu.VMEM(s, jnp.bfloat16) for s in scratch],
        compiler_params=pltpu.CompilerParams(vmem_limit_bytes=mib * 2**20),
        cost_estimate=pl.CostEstimate(
            flops=flops, bytes_accessed=2**20, transcendentals=0
        )
        if flops
        else None,
        **rest,
    )


def bf16(*shape):
    return jax.ShapeDtypeStruct(shape, jnp.bfloat16)


def join_kernel(a, b, out):
    n = a.shape[0]
    out[:n] = a[...]
    out[n:] = b[...]


def join(a, b):
    n = a.shape[0]
    return kernel_call(join_kernel, bf16(2 * n, 32, 512), 2)(a, b)


def stage_kernel(array, out):
    out[...] = array[...]


def norm_kernel(tokens, gain, normed, residual):
    mine = lax.axis_index("x") * CORE + lax.axis_index("core")
    residual[...] = tokens[pl.ds(pl.multiple_of(mine * 64, 64), 64), :]

    @pl.loop(0, 16)
    def _(n):
        rows = pl.ds(pl.multiple_of(n * 32, 32), 32)
        xf = tokens[rows, :].astype(jnp.float32)
        scale = lax.rsqrt(jnp.mean(xf * xf, axis=-1, keepdims=True) + EPS)
        normed[rows, :] = (xf * scale * gain[...]).astype(jnp.bfloat16)


def place(piece, laid, whole, halved):
    z, y = lax.axis_index("z"), lax.axis_index("y")
    sign = 2 * lax.axis_index("core") - 1
    for j, (dz, dy) in enumerate(laid):
        at_z = (z + sign * dz) & (Z - 1)
        at_y = (y + sign * dy) & (Y - 1)
        at = ((at_z >> 1) if halved else at_z) * Y + at_y
        whole[pl.ds(pl.multiple_of(at * 32, 32), 32), :] = piece[j]


def down_product(hidden, rows, down, out, part):
    @pl.loop(0, 4)
    def _(n):
        columns = pl.ds(pl.multiple_of(n * 256, 256), 256)
        out[part, :, columns] = lax.dot_general(
            hidden[rows, :],
            down[columns, :],
            (((1,), (1,)), ((), ())),
            preferred_element_type=jnp.float32,
        ).astype(jnp.bfloat16)


THEIRS, OWN = slice(0, 256), slice(256, 512)


def up_kernel(normed, u0, uz, uy, uzy, hidden, up):
    for piece, shift in ((u0, (0, 0)), (uz, (1, 0)), (uy, (0, 1)), (uzy, (1, 1))):
        place(piece, shifted(UP_STEPS, *shift), up, False)
    core = lax.axis_index("core")

    @pl.loop(0, 2)
    def _(n):
        columns = pl.ds(pl.multiple_of(n * 256, 256), 256)
        lifted = jnp.dot(
            normed[...], up[:, columns], preferred_element_type=jnp.float32
        )
        active = jnp.square(jnp.maximum(lifted, 0.0)).astype(jnp.bfloat16)
        for j in range(X * CORE):
            x, c = divmod(j, CORE)
            side = jnp.where(core == c, 256, 0)
            rows = pl.ds(pl.multiple_of(side + x * 64, 64), 64)
            hidden[rows, columns] = active[j * 64 : (j + 1) * 64]


def early_kernel(hidden, d0, dy, theirs, down):
    place(d0, offsets(DOWN_STEPS), down, True)
    place(dy, shifted(DOWN_STEPS, 0, 1), down, True)
    down_product(hidden, THEIRS, down, theirs, 0)


def late_kernel(hidden, dz, dyz, theirs_in, theirs, down):
    place(dz, shifted(DOWN_STEPS, 1, 0), down, True)
    place(dyz, shifted(DOWN_STEPS, 1, 1), down, True)
    down_product(hidden, THEIRS, down, theirs, 1)


def own_kernel(hidden, first, second, own):
    down_product(hidden, OWN, first, own, 0)
    down_product(hidden, OWN, second, own, 1)


def add_kernel(own, beside, ahead, near, keep, hold):
    x, core = lax.axis_index("x"), lax.axis_index("core")
    first, second = 1 + 2 * core, 3 - 2 * core
    for out, chunk in (
        (ahead, x ^ 2),
        (near, x ^ first),
        (keep, x),
        (hold, x ^ second),
    ):
        rows = pl.ds(pl.multiple_of(chunk * 64, 64), 64)
        for part in range(2):
            total = own[part, rows].astype(jnp.float32)
            total = total + beside[part, rows].astype(jnp.float32)
            out[part] = total.astype(jnp.bfloat16)


def pass_kernel(hold, came, out):
    total = hold[...].astype(jnp.float32) + came[...].astype(jnp.float32)
    out[...] = total.astype(jnp.bfloat16)


def last_kernel(residual, keep, came, late, out):
    odd = lax.axis_index("z") & 1
    for part in range(2):
        for k in range(4):
            at = (2 * k + (odd ^ part)) * 256
            columns = pl.ds(pl.multiple_of(at, 256), 256)
            here = slice(k * 256, (k + 1) * 256)
            total = residual[:, columns].astype(jnp.float32)
            for term in (keep, came, late):
                total = total + term[part, :, here].astype(jnp.float32)
            out[:, columns] = total.astype(jnp.bfloat16)


def gathered(up, down):
    for k in range(4):
        up_in = from_side(up, *UP_STEPS[k])
        down_in = from_side(down, *DOWN_STEPS[k])
        if k == 0:
            stage = kernel_call(stage_kernel, bf16(1, 32, 512), 1)
            up = stage(up)
            down = stage(down)
        up = join(up, up_in)
        down = join(down, down_in)
    up_z = from_side(up, "z", 1)
    up_y = from_side(up, "y", 1)
    down_y = from_side(down, "y", 1)
    down_z = from_side(down, "z", 1)
    up_zy = from_side(up_z, "y", 1)
    down_yz = from_side(down_y, "z", 1)
    return (up, up_z, up_y, up_zy), (down, down_y, down_z, down_yz)


def over_tp(beside, own, residual):
    piece = bf16(2, 64, 1024)
    ahead, near, keep, hold = kernel_call(add_kernel, (piece,) * 4, 2)(own, beside)
    through = between_x(ahead, 1, 3)
    came = between_x(near, 1, 3)
    passed = kernel_call(pass_kernel, piece, 2)(hold, through)
    late = between_x(passed, 3, 1)
    return kernel_call(last_kernel, bf16(64, 2048), 4)(residual, keep, came, late)


def shards(tokens, norm_gain, up_weight, down_weight):
    up, down = gathered(up_weight[None], down_weight.T[None])
    normed, residual = kernel_call(
        norm_kernel, (bf16(512, 2048), bf16(64, 2048)), 2, mib=12, flops=2**24
    )(tokens, norm_gain[None])
    hidden = kernel_call(
        up_kernel, bf16(512, 512), 5, scratch=((2048, 512),), mib=12, flops=2**30
    )(normed, *up)
    out, rows = bf16(2, 256, 1024), bf16(1024, 512)
    theirs, first = kernel_call(early_kernel, (out, rows), 3, flops=2**28)(
        hidden, *down[:2]
    )
    theirs, second = kernel_call(
        late_kernel,
        (out, rows),
        4,
        flops=2**28,
        input_output_aliases={3: 0},
    )(hidden, *down[2:], theirs)
    beside = lax.ppermute(theirs, "core", [(0, 1), (1, 0)])
    own = kernel_call(own_kernel, out, 3, flops=2**29)(hidden, first, second)
    return over_tp(beside, own, residual)


def solution(mesh):
    torus = Mesh(
        mesh.devices.reshape(REP, Z, Y, X, CORE), ("rep", "z", "y", "x", "core")
    )
    rep_fs = ("rep", "z", "y")
    tp = ("x", "core")
    in_specs = (P(rep_fs, None), P(), P(("z", "y"), tp), P(tp, ("z", "y")))
    return jax.shard_map(
        shards,
        mesh=torus,
        in_specs=in_specs,
        out_specs=P(rep_fs + tp, None),
        check_vma=False,
    )
```

```python
import jax
import jax.numpy as jnp
from jax import lax
from jax.experimental import pallas as pl
from jax.experimental.pallas import tpu as pltpu
from jax.sharding import Mesh
from jax.sharding import PartitionSpec as P


EPS = 1e-06
REP, Z, Y, X, CORE = 2, 8, 8, 4, 2
VMEM = pl.BlockSpec(memory_space=pltpu.VMEM)


UP_STEPS = (("z", 4), ("y", 4), ("y", 2), ("z", 2))
DOWN_STEPS = (("y", 4), ("z", 4), ("z", 2), ("y", 2))


def from_side(array, axis, shift):
    names, size = (("y", "core"), Y) if axis == "y" else (("rep", "z", "core"), REP * Z)
    pairs = []
    for i in range(size):
        pairs.append(((i + shift) % size * 2, i * 2))
        pairs.append(((i - shift) % size * 2 + 1, i * 2 + 1))
    return lax.ppermute(array, names, pairs)


def between_x(array, first, second):
    pairs = []
    for x in range(X):
        pairs.append((x * 2, (x ^ first) * 2))
        pairs.append((x * 2 + 1, (x ^ second) * 2 + 1))
    return lax.ppermute(array, ("x", "core"), pairs)


def offsets(steps):
    laid = [(0, 0)]
    for axis, shift in steps:
        dz, dy = (shift, 0) if axis == "z" else (0, shift)
        laid = laid + [(z + dz, y + dy) for z, y in laid]
    return laid


def shifted(steps, dz, dy):
    return [(z + dz, y + dy) for z, y in offsets(steps)]


def kernel_call(kernel, outs, n_vmem, scratch=(), mib=8, flops=0, **rest):
    single = not isinstance(outs, tuple)
    return pl.pallas_call(
        kernel,
        out_shape=outs,
        in_specs=[VMEM] * n_vmem,
        out_specs=VMEM if single else (VMEM,) * len(outs),
        scratch_shapes=[pltpu.VMEM(s, jnp.bfloat16) for s in scratch],
        compiler_params=pltpu.CompilerParams(vmem_limit_bytes=mib * 2**20),
        cost_estimate=pl.CostEstimate(
            flops=flops, bytes_accessed=2**20, transcendentals=0
        )
        if flops
        else None,
        **rest,
    )


def bf16(*shape):
    return jax.ShapeDtypeStruct(shape, jnp.bfloat16)


def join_kernel(a, b, out):
    n = a.shape[0]
    out[:n] = a[...]
    out[n:] = b[...]


def join(a, b):
    n = a.shape[0]
    return kernel_call(join_kernel, bf16(2 * n, 32, 512), 2)(a, b)


def stage_kernel(array, out):
    out[...] = array[...]


def norm_kernel(tokens, gain, normed, residual):
    mine = lax.axis_index("x") * CORE + lax.axis_index("core")
    residual[...] = tokens[pl.ds(pl.multiple_of(mine * 64, 64), 64), :]

    @pl.loop(0, 16)
    def _(n):
        rows = pl.ds(pl.multiple_of(n * 32, 32), 32)
        xf = tokens[rows, :].astype(jnp.float32)
        scale = lax.rsqrt(jnp.mean(xf * xf, axis=-1, keepdims=True) + EPS)
        normed[rows, :] = (xf * scale * gain[...]).astype(jnp.bfloat16)


def place(piece, laid, whole, halved):
    z, y = lax.axis_index("z"), lax.axis_index("y")
    sign = 1 - 2 * lax.axis_index("core")
    for j, (dz, dy) in enumerate(laid):
        at_z = (z + sign * dz) & (Z - 1)
        at_y = (y + sign * dy) & (Y - 1)
        at = ((at_z >> 1) if halved else at_z) * Y + at_y
        whole[pl.ds(pl.multiple_of(at * 32, 32), 32), :] = piece[j]


def down_product(hidden, rows, down, out, part):
    @pl.loop(0, 4)
    def _(n):
        columns = pl.ds(pl.multiple_of(n * 256, 256), 256)
        out[part, :, columns] = lax.dot_general(
            hidden[rows, :],
            down[columns, :],
            (((1,), (1,)), ((), ())),
            preferred_element_type=jnp.float32,
        ).astype(jnp.bfloat16)


THEIRS, OWN = slice(0, 256), slice(256, 512)


def up_kernel(normed, u0, uz, uy, uzy, hidden, up):
    for piece, shift in ((u0, (0, 0)), (uz, (1, 0)), (uy, (0, 1)), (uzy, (1, 1))):
        place(piece, shifted(UP_STEPS, *shift), up, False)
    core = lax.axis_index("core")

    @pl.loop(0, 2)
    def _(n):
        columns = pl.ds(pl.multiple_of(n * 256, 256), 256)
        lifted = jnp.dot(
            normed[...], up[:, columns], preferred_element_type=jnp.float32
        )
        active = jnp.square(jnp.maximum(lifted, 0.0)).astype(jnp.bfloat16)
        for j in range(X * CORE):
            x, c = divmod(j, CORE)
            side = jnp.where(core == c, 256, 0)
            rows = pl.ds(pl.multiple_of(side + x * 64, 64), 64)
            hidden[rows, columns] = active[j * 64 : (j + 1) * 64]


def early_kernel(hidden, d0, dy, theirs, down):
    place(d0, offsets(DOWN_STEPS), down, True)
    place(dy, shifted(DOWN_STEPS, 0, 1), down, True)
    down_product(hidden, THEIRS, down, theirs, 0)


def late_kernel(hidden, dz, dyz, theirs_in, theirs, down):
    place(dz, shifted(DOWN_STEPS, 1, 0), down, True)
    place(dyz, shifted(DOWN_STEPS, 1, 1), down, True)
    down_product(hidden, THEIRS, down, theirs, 1)


def own_kernel(hidden, first, second, own):
    down_product(hidden, OWN, first, own, 0)
    down_product(hidden, OWN, second, own, 1)


def add_kernel(own, beside, ahead, near, keep, hold):
    x, core = lax.axis_index("x"), lax.axis_index("core")
    first, second = 1 + 2 * core, 3 - 2 * core
    for out, chunk in (
        (ahead, x ^ 2),
        (near, x ^ first),
        (keep, x),
        (hold, x ^ second),
    ):
        rows = pl.ds(pl.multiple_of(chunk * 64, 64), 64)
        for part in range(2):
            total = own[part, rows].astype(jnp.float32)
            total = total + beside[part, rows].astype(jnp.float32)
            out[part] = total.astype(jnp.bfloat16)


def pass_kernel(hold, came, out):
    total = hold[...].astype(jnp.float32) + came[...].astype(jnp.float32)
    out[...] = total.astype(jnp.bfloat16)


def last_kernel(residual, keep, came, late, out):
    odd = lax.axis_index("z") & 1
    for part in range(2):
        for k in range(4):
            at = (2 * k + (odd ^ part)) * 256
            columns = pl.ds(pl.multiple_of(at, 256), 256)
            here = slice(k * 256, (k + 1) * 256)
            total = residual[:, columns].astype(jnp.float32)
            for term in (keep, came, late):
                total = total + term[part, :, here].astype(jnp.float32)
            out[:, columns] = total.astype(jnp.bfloat16)


def gathered(up, down):
    for k in range(4):
        up_in = from_side(up, *UP_STEPS[k])
        down_in = from_side(down, *DOWN_STEPS[k])
        if k == 0:
            stage = kernel_call(stage_kernel, bf16(1, 32, 512), 1)
            up = stage(up)
            down = stage(down)
        up = join(up, up_in)
        down = join(down, down_in)
    up_z = from_side(up, "z", 1)
    up_y = from_side(up, "y", 1)
    down_y = from_side(down, "y", 1)
    down_z = from_side(down, "z", 1)
    up_zy = from_side(up_z, "y", 1)
    down_yz = from_side(down_y, "z", 1)
    return (up, up_z, up_y, up_zy), (down, down_y, down_z, down_yz)


def over_tp(beside, own, residual):
    piece = bf16(2, 64, 1024)
    ahead, near, keep, hold = kernel_call(add_kernel, (piece,) * 4, 2)(own, beside)
    through = between_x(ahead, 1, 3)
    came = between_x(near, 1, 3)
    passed = kernel_call(pass_kernel, piece, 2)(hold, through)
    late = between_x(passed, 3, 1)
    return kernel_call(last_kernel, bf16(64, 2048), 4)(residual, keep, came, late)


def shards(tokens, norm_gain, up_weight, down_weight):
    up, down = gathered(up_weight[None], down_weight.T[None])
    normed, residual = kernel_call(
        norm_kernel, (bf16(512, 2048), bf16(64, 2048)), 2, mib=12, flops=2**24
    )(tokens, norm_gain[None])
    hidden = kernel_call(
        up_kernel, bf16(512, 512), 5, scratch=((2048, 512),), mib=12, flops=2**30
    )(normed, *up)
    out, rows = bf16(2, 256, 1024), bf16(1024, 512)
    theirs, first = kernel_call(early_kernel, (out, rows), 3, flops=2**28)(
        hidden, *down[:2]
    )
    theirs, second = kernel_call(
        late_kernel,
        (out, rows),
        4,
        flops=2**28,
        input_output_aliases={3: 0},
    )(hidden, *down[2:], theirs)
    beside = lax.ppermute(theirs, "core", [(0, 1), (1, 0)])
    own = kernel_call(own_kernel, out, 3, flops=2**29)(hidden, first, second)
    return over_tp(beside, own, residual)


def solution(mesh):
    torus = Mesh(
        mesh.devices.reshape(REP, Z, Y, X, CORE), ("rep", "z", "y", "x", "core")
    )
    rep_fs = ("rep", "z", "y")
    tp = ("x", "core")
    in_specs = (P(rep_fs, None), P(), P(("z", "y"), tp), P(tp, ("z", "y")))
    return jax.shard_map(
        shards,
        mesh=torus,
        in_specs=in_specs,
        out_specs=P(rep_fs + tp, None),
        check_vma=False,
    )
```
